32 devices in a mesh: ep: 4 (over y, x), tp: 8 (over z, core).
Axes of the slice: x: 2, y: 2, z: 4, core: 2. Of those that a mesh axis runs over, the one named last changes fastest.
Arguments:
- mix_tokens: bfloat16 [512, 4096], P('ep'), may hold values from -6 to 6
- mix_gain: float32 [4096], replicated, may hold values from 0.1 to 1.9
- value_weight: bfloat16 [4096, 2048], P(None, 'tp'), may hold values from -0.09375 to 0.09375
- inner_weight: bfloat16 [4096, 2048], P(None, 'tp'), may hold values from -0.09375 to 0.09375
- outer_weight: bfloat16 [4096, 2048], P(None, 'tp'), may hold values from -0.09375 to 0.09375
- conv_taps: float32 [3, 2048], P(None, 'tp'), may hold values from -3 to 3
- mix_weight: bfloat16 [2048, 4096], P('tp'), may hold values from -0.125 to 0.125
- moe_tokens: bfloat16 [512, 4096], P('ep'), may hold values from -6 to 6
- moe_gain: float32 [4096], replicated, may hold values from 0.1 to 1.9
- router_group: bfloat16 [4096, 4], replicated, may hold values from -0.09375 to 0.09375
- router_expert: bfloat16 [4096, 16], replicated, may hold values from -0.09375 to 0.09375
- expert_routes: int32 [512, 2], P('ep'), may hold values from 0 to 15, as said below
- gate_weight: bfloat16 [16, 4096, 2048], P('ep', None, 'tp'), may hold values from -0.09375 to 0.09375
- up_weight: bfloat16 [16, 4096, 2048], P('ep', None, 'tp'), may hold values from -0.09375 to 0.09375
- down_weight: bfloat16 [16, 2048, 4096], P('ep', 'tp'), may hold values from -0.5 to 0.5
Outputs:
- mixer_out: bfloat16 [512, 4096], P(('ep', 'tp'))
- expert_out: bfloat16 [512, 4096], P(('ep', 'tp'))
The draws below stay inside these ranges and needn't reach their ends.
Inputs may be any that keep to these rules, and one draw needn't show every extreme that they name: `expert_routes`: the two experts of a row are different and lie in one group of 4 consecutive expert numbers. In each aligned block of 16 rows no expert is named more than 4 times, and in every draw some experts are named exactly 4 times in every block.
All inputs are finite; a program needn't handle non-finite values.
Results may differ from the reference program's by a relative error of at most 0.0076.
Values may be sent and summed in bfloat16 or wider, within the bound.
A program may use at most 128 MiB of HBM per device.

```python
import jax
import jax.numpy as jnp
from jax import lax

D = 4096
CONV_CH = 2048
TAPS = 3
FE = 2048
EXPERTS = 16
GROUPS = 4
TOPK = 2
MOE_SHARE = 16
EPG = 4
CAP = 4
MIX_TOKENS = 512
MOE_TOKENS = 512


def draw_expert_routes(key, part):
    blocks = MOE_TOKENS // MOE_SHARE
    half_share = MOE_SHARE // 2
    subkeys = jax.random.split(jax.random.fold_in(key, 7), 5)
    hot_group = jax.random.randint(subkeys[0], (), 0, GROUPS).astype(jnp.int32)
    others = (hot_group + 1 + jax.random.randint(subkeys[1], (blocks, MOE_SHARE - half_share), 0, GROUPS - 1)) % GROUPS
    labels = jnp.concatenate([jnp.full((blocks, half_share), hot_group, jnp.int32), others.astype(jnp.int32)], axis=1)
    scores = jax.random.randint(subkeys[2], (blocks, MOE_SHARE), 0, 1048576) * MOE_SHARE + jnp.arange(MOE_SHARE, dtype=jnp.int32)[None, :]
    ordering = jnp.argsort(scores, axis=1, stable=True)
    labels = jnp.take_along_axis(labels, ordering, axis=1)
    one_hot = (labels[:, :, None] == jnp.arange(GROUPS, dtype=jnp.int32)[None, None, :]).astype(jnp.int32)
    within = jnp.sum((jnp.cumsum(one_hot, axis=1) - one_hot) * one_hot, axis=2)
    offsets = jax.random.randint(subkeys[3], (blocks, GROUPS), 0, EPG)
    strides = jax.random.randint(subkeys[4], (blocks, GROUPS), 1, EPG)
    offset_tok = jnp.take_along_axis(offsets, labels, axis=1)
    stride_tok = jnp.take_along_axis(strides, labels, axis=1)
    first_pick = labels * EPG + (within + offset_tok) % EPG
    second_pick = labels * EPG + (within + offset_tok + stride_tok) % EPG
    return jnp.stack([first_pick, second_pick], axis=-1).reshape(blocks * MOE_SHARE, TOPK).astype(jnp.int32)


def levels(rng, shape, cuts, smallest, top_value):
    loudness = 1.0
    for dim, shards_of in cuts:
        draws = jax.random.uniform(jax.random.fold_in(jax.random.fold_in(rng, 6), dim), (shards_of,), jnp.float32, smallest / len(cuts), top_value / len(cuts))
        loudness = loudness * jnp.repeat(jnp.exp(draws), shape[dim] // shards_of).reshape((-1,) + (1,) * (len(shape) - 1 - dim))
    return loudness


def bell_draw(own_key, dims, deviation, limit, cuts=(), kind=jnp.bfloat16):
    values = deviation * jax.random.normal(own_key, dims, jnp.float32)
    if cuts:
        values = values * levels(own_key, dims, cuts, -0.22, 0.18)
    return jnp.clip(values, -limit, limit).astype(kind)


def setup_inputs(seed: int = 0) -> dict:
    seeds = jax.random.split(jax.random.key(seed), 16)
    return {
        "mix_tokens": bell_draw(seeds[0], (MIX_TOKENS, D), 1.0, 6.0, ((0, 4),)),
        "mix_gain": jnp.clip(1.0 + 0.18 * jax.random.normal(seeds[1], (D,), jnp.float32), 0.1, 1.9),
        "value_weight": bell_draw(seeds[2], (D, CONV_CH), D ** -0.5, 0.09375, ((1, 8),)),
        "inner_weight": bell_draw(seeds[3], (D, CONV_CH), D ** -0.5, 0.09375, ((1, 8),)),
        "outer_weight": bell_draw(seeds[4], (D, CONV_CH), D ** -0.5, 0.09375, ((1, 8),)),
        "conv_taps": bell_draw(seeds[5], (TAPS, CONV_CH), 0.6, 3.0, ((1, 8),), jnp.float32),
        "mix_weight": bell_draw(seeds[6], (CONV_CH, D), CONV_CH ** -0.5, 0.125, ((0, 8),)),
        "moe_tokens": bell_draw(seeds[7], (MOE_TOKENS, D), 1.0, 6.0, ((0, 4),)),
        "moe_gain": jnp.clip(1.0 + 0.18 * jax.random.normal(seeds[8], (D,), jnp.float32), 0.1, 1.9),
        "router_group": bell_draw(seeds[9], (D, GROUPS), D ** -0.5, 0.09375),
        "router_expert": bell_draw(seeds[10], (D, EXPERTS), D ** -0.5, 0.09375),
        "expert_routes": draw_expert_routes(jax.random.fold_in(seeds[15], 71), 0),
        "gate_weight": bell_draw(seeds[12], (EXPERTS, D, FE), D ** -0.5, 0.09375, ((0, 4), (2, 8))),
        "up_weight": bell_draw(seeds[13], (EXPERTS, D, FE), D ** -0.5, 0.09375, ((0, 4), (2, 8))),
        "down_weight": bell_draw(seeds[14], (EXPERTS, FE, D), (FE // 16) ** -0.5, 0.5, ((0, 4), (1, 8))),
    }


def rms_rows(inputs, gain_vec):
    values = inputs.astype(jnp.float32)
    inverse = lax.rsqrt(lax.optimization_barrier(jnp.mean(values * values, axis=-1, keepdims=True)) + 1e-06)
    return (values * inverse * gain_vec.astype(jnp.float32)).astype(jnp.bfloat16)

def route_weights(normed, routes, router_group, router_expert):
    group_logit = jnp.dot(normed, router_group, preferred_element_type=jnp.float32)
    expert_logit = jnp.dot(normed, router_expert, preferred_element_type=jnp.float32)
    group_exp = jnp.exp(group_logit)
    group_id = routes[:, 0] // EPG
    group_pick = (group_id[:, None] == jnp.arange(GROUPS, dtype=jnp.int32)[None, :]).astype(jnp.float32)
    group_gate = lax.optimization_barrier(jnp.sum(group_exp * group_pick, axis=1)) / lax.optimization_barrier(jnp.sum(group_exp, axis=1))
    expert_pick = (routes[:, :, None] == jnp.arange(EXPERTS, dtype=jnp.int32)[None, None, :]).astype(jnp.float32)
    chosen = jnp.exp(lax.optimization_barrier(jnp.sum(expert_logit[:, None, :] * expert_pick, axis=2)))
    return group_gate[:, None] * chosen / lax.optimization_barrier(jnp.sum(chosen, axis=1, keepdims=True))

def slot_ranks(routes):
    blocks = routes.shape[0] // MOE_SHARE
    entries = routes.reshape(blocks, MOE_SHARE * TOPK)
    one_hot = (entries[:, :, None] == jnp.arange(EXPERTS, dtype=jnp.int32)[None, None, :]).astype(jnp.int32)
    before = jnp.cumsum(one_hot, axis=1) - one_hot
    return lax.optimization_barrier(jnp.sum(before * one_hot, axis=2)).reshape(routes.shape)

def reference(mix_tokens, mix_gain, value_weight, inner_weight, outer_weight, conv_taps, mix_weight, moe_tokens, moe_gain, router_group, router_expert, expert_routes, gate_weight, up_weight, down_weight):
    normed = rms_rows(mix_tokens, mix_gain)
    value_proj = jnp.dot(normed, value_weight, preferred_element_type=jnp.float32)
    inner_proj = jnp.dot(normed, inner_weight, preferred_element_type=jnp.float32)
    outer_proj = jnp.dot(normed, outer_weight, preferred_element_type=jnp.float32)
    gated_in = lax.optimization_barrier((inner_proj * value_proj).astype(jnp.bfloat16)).astype(jnp.float32)
    seq_rows = gated_in.shape[0]
    padded = jnp.concatenate([jnp.zeros((TAPS - 1, gated_in.shape[1]), jnp.float32), gated_in], axis=0)
    tap_values = conv_taps.astype(jnp.float32)
    mixed_conv = tap_values[0] * padded[0:seq_rows]
    for tap_index in range(1, TAPS):
        mixed_conv = mixed_conv + tap_values[tap_index] * padded[tap_index:tap_index + seq_rows]
    conv_out = (outer_proj * mixed_conv).astype(jnp.bfloat16)
    mixer_out = jnp.dot(conv_out, mix_weight, preferred_element_type=jnp.float32).astype(jnp.bfloat16)
    moe_normed = rms_rows(moe_tokens, moe_gain)
    weights = route_weights(moe_normed, expert_routes, router_group, router_expert)
    ranks = slot_ranks(expert_routes)
    total_rows = moe_tokens.shape[0]
    block_id = jnp.arange(total_rows, dtype=jnp.int32) // MOE_SHARE
    position = (block_id[:, None] * CAP + ranks).astype(jnp.int32)
    per_expert = total_rows // MOE_SHARE * CAP
    token_id = jnp.broadcast_to(jnp.arange(total_rows, dtype=jnp.int32)[:, None], (total_rows, TOPK))
    slot_table = jnp.zeros((EXPERTS, per_expert), jnp.int32).at[expert_routes, position].set(token_id)

    def run_expert(operands):
        row_index, gate_w, up_w, down_w = operands
        picked_rows = moe_normed[row_index]
        gate_proj = jnp.dot(picked_rows, gate_w, preferred_element_type=jnp.float32)
        up_proj = jnp.dot(picked_rows, up_w, preferred_element_type=jnp.float32)
        hidden = (jax.nn.silu(gate_proj) * up_proj).astype(jnp.bfloat16)
        summed = jnp.dot(hidden, down_w, preferred_element_type=jnp.float32)
        return summed.astype(jnp.bfloat16)
    results = lax.map(run_expert, (slot_table, gate_weight, up_weight, down_weight))
    picked = results[expert_routes, position].astype(jnp.float32)
    expert_out = lax.optimization_barrier(jnp.sum(weights[:, :, None] * picked, axis=1)).astype(jnp.bfloat16)
    return (mixer_out, expert_out)
```

```python
import functools

import jax
import jax.numpy as jnp
from jax import lax
from jax.experimental import pallas as pl
from jax.experimental.pallas import tpu as pltpu
from jax.sharding import PartitionSpec as P

EPG = 4
CAP = 4
CORES = 2
CHUNKS = (1, 2, 2, 2, 2, 2, 2, 2, 1)
LAGS = (2, 8, 2, 3)
DIRECT = 2
SPLIT = (2, 2, 3, 1)
PARTS = len(SPLIT)
MESH = pl.DeviceIdType.MESH
F32, BF16 = jnp.float32, jnp.bfloat16


def iota(shape, dim):
    return lax.broadcasted_iota(jnp.int32, shape, dim)


def norm_rows(src, gain, dst):
    width = src.shape[1]

    def body(i, carry):
        rows = pl.ds(pl.multiple_of(i * 16, 16), 16)
        x = src[rows, :].astype(F32)
        inv = lax.rsqrt(jnp.sum(x * x, axis=1, keepdims=True) * (1.0 / width) + 1e-06)
        dst[rows, :] = (x * inv * gain[...]).astype(BF16)
        return carry

    lax.fori_loop(0, src.shape[0] // 16, body, 0, unroll=4)


def row_scales(src):
    width = src.shape[1]
    total = None
    for first in range(0, width, 512):
        x = src[:, first : first + 512].astype(F32)
        square = x * x
        total = square if total is None else total + square
    return lax.rsqrt(jnp.sum(total, axis=1, keepdims=True) * (1.0 / width) + 1e-06)


def column_tiles(width, tile, body):
    def step(i, carry):
        body(pl.ds(pl.multiple_of(i * tile, tile), tile))
        return carry

    lax.fori_loop(0, width // tile, step, 0)


def kernel(
    cfg,
    mix_tokens, mix_gain_in, value_w, inner_w, outer_w, taps_in, mix_w, moe_tokens, moe_gain_in,
    router_group, router_expert, routes_in, gate_w, up_w, down_w,
    mixer_out, expert_out,
    mix_gain, taps, moe_gain, routes, xm, xe, rg, rx, vw, iw, ow, mw, gw, uw, dw,
    nm, ne, spread, gather, pack, got, wpack, wgot, wrow,
    gated, halo, padded, conv, ordered, pair_out, pair_in, keep, zin,
    gate_acc, up_acc, hid, both_y, y_out, y_in, y_keep, e_in, s_keep, s_out, s_in,
    load_sem, expert_sem, down_sem,
    near_s, near_r, far_s, far_r, rel_s, rel_r, w_s, w_r, fwd_s, fwd_r, halo_s, halo_r,
    mp_s, mp_r, mz_s, mz_r, yp_s, yp_r, ye_s, ye_r, yz_s, yz_r,
):
    ep, side, tp, zs, half, experts_here, w_rows = cfg
    e_me, t_me = lax.axis_index("ep"), lax.axis_index("tp")
    z_me, c_me = t_me // CORES, lax.rem(t_me, CORES)
    c_no = 1 - c_me
    partner = z_me * CORES + c_no
    width = xm.shape[1]
    tall = ep // side
    e_row, e_col = e_me // side, lax.rem(e_me, side)

    def placed(down, across):
        return lax.rem(e_row + down, tall) * side + lax.rem(e_col + across, side)

    near = [placed(d, 0) for d in range(1, tall)] + [placed(0, a) for a in range(1, side)]
    far = [placed(d, a) for d in range(1, tall) for a in range(1, side)]
    ep_peers = near + far
    z_odd = lax.rem(z_me, 2)
    z_pair = z_me + 1 - 2 * z_odd
    z_peers = [lax.rem(z_me + d, zs) for d in range(1, zs)]

    def start(copy):
        copy.start()

    barrier = pltpu.get_barrier_semaphore()
    for e in ep_peers:
        pl.semaphore_signal(barrier, inc=1, device_id={"ep": e, "tp": t_me}, device_id_type=MESH)
    for z in z_peers:
        pl.semaphore_signal(
            barrier, inc=1, device_id={"ep": e_me, "tp": z * CORES + c_me}, device_id_type=MESH
        )
    pl.semaphore_signal(barrier, inc=1, device_id={"ep": e_me, "tp": partner}, device_id_type=MESH)

    def load(k, src, dst):
        return pltpu.make_async_copy(src, dst, load_sem.at[k])

    loads = [
        load(k, s, d)
        for k, (s, d) in enumerate(
            [
                (moe_tokens, xe), (router_group, rg), (router_expert, rx), (mix_tokens, xm),
                (value_w, vw), (inner_w, iw), (outer_w, ow), (mix_w, mw),
                (routes_in, routes), (moe_gain_in, moe_gain), (mix_gain_in, mix_gain), (taps_in, taps),
            ]
        )
    ]
    unit = width // sum(SPLIT)

    def part_slice(q):
        return sum(SPLIT[:q]) * unit, SPLIT[q] * unit

    def expert_loads(q):
        rows = pl.ds(*part_slice(q))
        return [
            pltpu.make_async_copy(gate_w.at[:, rows, :], gw.at[:, rows, :], expert_sem.at[q]),
            pltpu.make_async_copy(up_w.at[:, rows, :], uw.at[:, rows, :], expert_sem.at[q]),
        ]

    hidden = down_w.shape[1]
    down_loads = [
        pltpu.make_async_copy(
            down_w.at[k], dw.at[k * hidden : (k + 1) * hidden, :], down_sem
        )
        for k in range(experts_here)
    ]
    for k in (8, 0, 9, 3, 10, 4, 5):
        loads[k].start()

    def remote(src, dst, s_sem, r_sem, e, t):
        return pltpu.make_async_remote_copy(
            src_ref=src, dst_ref=dst, send_sem=s_sem, recv_sem=r_sem,
            device_id={"ep": e, "tp": t}, device_id_type=MESH,
        )

    count = xe.shape[0]
    share = count // tp
    slots = half // zs
    span = ep * half
    loads[8].wait()
    diagonal = jnp.where(iota((count, count), 0) == iota((count, count), 1), 1.0, 0.0)
    r = lax.dot_general(
        diagonal.astype(BF16), routes[...].astype(F32).astype(BF16), (((1,), (1,)), ((), ())),
        preferred_element_type=F32,
    ).astype(jnp.int32)
    picks = [r[:, 0:1], r[:, 1:2]]
    lane = iota((count, -(-ep * w_rows // 128) * 128), 1)
    shards = [
        sum((p >= s * experts_here).astype(jnp.int32) for s in range(1, ep)) for p in picks
    ]
    member = jnp.where((lane == shards[0]) | (lane == shards[1]), 1.0, 0.0).astype(BF16)
    ti, tj = iota((count, count), 0), iota((count, count), 1)
    earlier = jnp.where(((ti ^ tj) < share) & (tj < ti), 1.0, 0.0).astype(BF16)
    rank = jnp.dot(earlier, member, preferred_element_type=F32)
    block = lax.shift_right_logical(iota((count, 1), 0), share.bit_length() - 1)
    base = (block & 1) * span + lax.shift_right_logical(block, 1) * slots
    slot_lane = iota((count, 2 * span), 1)
    hits = []
    for s in shards:
        mine = jnp.sum(jnp.where(lane == s, rank, 0.0), axis=1, keepdims=True).astype(jnp.int32)
        hits.append(slot_lane == base + s * half + mine)
    one_hot = jnp.where(hits[0] | hits[1], 1.0, 0.0).astype(BF16)
    spread[...] = one_hot
    gather[...] = lax.dot_general(
        one_hot, diagonal.astype(BF16), (((0,), (0,)), ((), ())), preferred_element_type=F32
    ).astype(BF16)
    loads[0].wait()
    loads[9].wait()

    def pack_part(q):
        first, size = part_slice(q)
        cols = slice(first, first + size)
        ne[:, cols] = (xe[:, cols].astype(F32) * moe_gain[:, cols]).astype(BF16)
        pack[:, cols] = jnp.dot(
            gather[...], ne[:, cols], preferred_element_type=F32
        ).astype(BF16)

    pack_part(0)
    pack_part(1)
    for k in (1, 2, 6, 11, 7):
        loads[k].start()
    for c in expert_loads(0):
        c.start()
    pl.semaphore_wait(barrier, (ep - 1) + (zs - 1) + 1)
    def half_rows(c, e):
        return pl.ds(pl.multiple_of(c * span + e * half, half), half)

    def half_cols(q, odd):
        first, size = part_slice(q)
        return pl.ds(pl.multiple_of(first + odd * (size // 2), 128), size // 2)

    def dispatch(q, peers, cols, s_sem, r_sem):
        for e in peers:
            start(
                remote(
                    pack.at[half_rows(c_me, e), cols], got.at[half_rows(c_me, e_me), cols],
                    s_sem, r_sem.at[q], e, t_me,
                )
            )

    def dispatch_far(q):
        dispatch(q, far, half_cols(q, z_odd), far_s, far_r)

    def dispatch_near(q):
        dispatch(q, near, pl.ds(*part_slice(q)), near_s, near_r)

    def landed(count, size, sem):
        here = got.at[pl.ds(0, count * half), pl.ds(0, size)]
        remote(here, here, sem, sem, e_me, partner).wait_recv()

    def forward(q, e, cols):
        here = got.at[half_rows(c_me, e), cols]
        start(remote(here, here, fwd_s, fwd_r.at[q], e_me, partner))

    def relay(q):
        cols = half_cols(q, z_odd)
        landed(len(far), part_slice(q)[1] // 2, far_r.at[q])
        for e in far:
            here = got.at[half_rows(c_me, e), cols]
            start(remote(here, here, rel_s, rel_r.at[q], e_me, z_pair * CORES + c_me))
            forward(q, e, cols)

    def forward_near(q):
        landed(len(near), part_slice(q)[1], near_r.at[q])
        for e in near:
            forward(q, e, pl.ds(*part_slice(q)))

    def forward_far(q):
        landed(len(far), part_slice(q)[1] // 2, rel_r.at[q])
        for e in far:
            forward(q, e, half_cols(q, 1 - z_odd))

    def forwarded(q):
        landed(ep - 1, part_slice(q)[1], fwd_r.at[q])

    dispatch_far(0)
    dispatch_near(0)
    loads[3].wait()
    loads[10].wait()
    norm_rows(xm, mix_gain, nm)
    loads[4].wait()
    loads[5].wait()
    rows = xm.shape[0]
    value_proj = jnp.dot(nm[...], vw[...], preferred_element_type=F32)
    inner_proj = jnp.dot(nm[...], iw[...], preferred_element_type=F32)
    gated[...] = (inner_proj * value_proj).astype(BF16)
    halo_copy = remote(
        gated.at[pl.ds(rows - 16, 16), :], halo, halo_s, halo_r,
        lax.rem(e_me + 1, ep), t_me,
    )
    halo_copy.start()
    dispatch_far(1)
    for q in range(1, PARTS):
        for c in expert_loads(q):
            c.start()
    for q in range(2, PARTS):
        pack_part(q)
        dispatch_far(q)
        dispatch_near(q - 1)
    loads[1].wait()
    loads[2].wait()
    lanes = (((1,), (1,)), ((), ()))
    row_scale = row_scales(xe)
    group_exp = jnp.exp(
        row_scale * lax.dot_general(ne[...], rg[...], lanes, preferred_element_type=F32)
    )
    expert_logit = row_scale * lax.dot_general(
        ne[...], rx[...], lanes, preferred_element_type=F32
    )
    groups, experts = group_exp.shape[1], expert_logit.shape[1]
    group = sum((picks[0] >= s * EPG).astype(jnp.int32) for s in range(1, groups))
    chosen_group = jnp.where(iota((count, groups), 1) == group, group_exp, 0.0)
    group_gate = jnp.sum(chosen_group, axis=1, keepdims=True) / jnp.sum(
        group_exp, axis=1, keepdims=True
    )
    expert_lane = iota((count, experts), 1)
    chosen = [
        jnp.exp(jnp.sum(jnp.where(expert_lane == p, expert_logit, 0.0), axis=1, keepdims=True))
        for p in picks
    ]
    scale = chosen[0] + chosen[1]
    w_lanes = [s * w_rows + (p - s * experts_here) for s, p in zip(shards, picks)]
    weights = sum(
        jnp.where(lane == at, group_gate * c / scale, 0.0) for at, c in zip(w_lanes, chosen)
    )
    scale_lanes = [s * w_rows + experts_here for s in shards]
    weights = weights + jnp.where(
        (lane == scale_lanes[0]) | (lane == scale_lanes[1]), row_scale, 0.0
    )

    def three_parts(value):
        parts = []
        for _ in range(3):
            parts.append(value.astype(BF16))
            value = value - parts[-1].astype(F32)
        return parts

    packed_w = sum(
        lax.dot_general(p, spread[...], (((0,), (0,)), ((), ())), preferred_element_type=F32)
        for p in three_parts(weights)
    )
    for e in range(ep):
        for c in range(CORES):
            wpack[e, :, c * half : (c + 1) * half] = packed_w[
                e * w_rows : (e + 1) * w_rows, c * span + e * half : c * span + (e + 1) * half
            ]
    wgot[e_me] = wpack[e_me]
    for c in range(CORES):
        got[half_rows(c, e_me), :] = pack[half_rows(c, e_me), :]

    for e in ep_peers:
        start(remote(wpack.at[e], wgot.at[e_me], w_s, w_r, e, t_me))
    dispatch_near(PARTS - 1)
    padded[8:, :] = gated[...].astype(F32)
    loads[6].wait()
    outer_proj = jnp.dot(nm[...], ow[...], preferred_element_type=F32)
    mix_share = rows // tp
    mix_rows = zs * mix_share
    everything = slice(None)
    pair_copy = remote(pair_out, pair_in, mp_s, mp_r, e_me, partner)

    def parity_rows(ref, c, step, cols):
        return jnp.concatenate(
            [
                ref[pl.ds(pl.multiple_of((z * CORES + c) * step, step), step), cols]
                for z in range(zs)
            ],
            axis=0,
        )

    def z_rows(z, step):
        return pl.ds(pl.multiple_of(z * step, step), step)

    steps = zs.bit_length() - 1

    def z_partner(s):
        return z_me + (1 - 2 * lax.rem(z_me // 2**s, 2)) * 2**s

    def z_owners(z, s):
        low = lax.rem(z, 2 ** (s + 1))
        return [low + m * 2 ** (s + 1) for m in range(zs >> (s + 1))]

    def z_slot(s):
        return sum(zs >> (t + 1) for t in range(s))

    def z_send(s, src, dst, step, cols, s_sem, r_sem):
        to = z_partner(s)
        for m, owner in enumerate(z_owners(to, s)):
            start(
                remote(
                    src.at[z_rows(owner, step), cols], dst.at[z_slot(s) + m, :, cols],
                    s_sem, r_sem, e_me, to * CORES + c_me,
                )
            )

    def z_landed(blocks, ref, size, sem):
        here = ref.at[pl.ds(0, blocks), :, pl.ds(0, size)]
        remote(here, here, sem, sem, e_me, partner).wait_recv()

    def mixer_pair():
        halo_copy.wait()
        before = halo[...].astype(F32)[8:16, :]
        padded[0:8, :] = jnp.where(e_me > 0, before, jnp.zeros_like(before))
        loads[11].wait()
        n_taps = taps.shape[0]
        mixed = taps[0:1, :] * padded[pl.ds(9 - n_taps, rows), :]
        for j in range(1, n_taps):
            mixed = mixed + taps[j : j + 1, :] * padded[pl.ds(9 - n_taps + j, rows), :]
        conv[...] = (outer_proj * mixed).astype(BF16)

        loads[7].wait()

        ordered[0:mix_rows, :] = parity_rows(conv, c_no, mix_share, everything)
        ordered[mix_rows:, :] = parity_rows(conv, c_me, mix_share, everything)

        def mix_tile(cols):
            both = jnp.dot(ordered[...], mw[:, cols], preferred_element_type=F32)
            pair_out[:, cols] = both[0:mix_rows].astype(BF16)
            keep[:, cols] = both[mix_rows:]

        column_tiles(width, 512, mix_tile)
        pair_copy.start()

    def mixer_sums():
        pair_copy.wait_recv()

        def sum_tile(cols):
            total = keep[:, cols] + pair_in[:, cols].astype(F32)
            keep[:, cols] = total
            pair_in[:, cols] = total.astype(BF16)

        column_tiles(width, 512, sum_tile)

        z_send(0, pair_in, zin, mix_share, pl.ds(0, width), mz_s, mz_r.at[0])

    def mixer_step(s):
        z_landed(zs >> s, zin, width, mz_r.at[s - 1])
        for m, owner in enumerate(z_owners(z_me, s - 1)):
            rows = z_rows(owner, mix_share)
            total = keep[rows, :] + zin[z_slot(s - 1) + m].astype(F32)
            keep[rows, :] = total
            pair_in[rows, :] = total.astype(BF16)
        z_send(s, pair_in, zin, mix_share, pl.ds(0, width), mz_s, mz_r.at[s])

    def project(q):
        first, size = part_slice(q)
        cols = slice(first, first + size)

        for k in range(experts_here):
            gate = jnp.dot(got[:, cols], gw[k, cols, :], preferred_element_type=F32)
            up = jnp.dot(got[:, cols], uw[k, cols, :], preferred_element_type=F32)
            if q:
                gate = gate + gate_acc[k]
                up = up + up_acc[k]
            if q < PARTS - 1:
                gate_acc[k] = gate
                up_acc[k] = up
                continue
            row = wrow[:, experts_here : experts_here + 1]
            gate = gate * row
            hid[:, k * hidden : (k + 1) * hidden] = (gate / (1.0 + jnp.exp(-gate)) * up * (row * wrow[:, k : k + 1])).astype(BF16)

    def arrived_weights():
        arrived = wgot.at[pl.ds(0, ep - 1)]
        remote(arrived, arrived, w_s, w_r, e_me, partner).wait_recv()
        across = jnp.concatenate(
            [wgot[e, :, c * half : (c + 1) * half] for c in range(CORES) for e in range(ep)], axis=1
        )
        square = (2 * span, 2 * span)
        same = jnp.where(iota(square, 0) == iota(square, 1), 1.0, 0.0).astype(BF16)
        wrow[...] = sum(
            lax.dot_general(same, p, lanes, preferred_element_type=F32)
            for p in three_parts(across)
        )

    for c in down_loads:
        c.start()
    relay(0)
    forward_near(0)
    relay(1)
    mixer_pair()
    forward_far(0)
    for q in range(PARTS):
        if q == 1:
            for later in range(2, PARTS):
                relay(later)
            mixer_sums()
        if q == 2:
            arrived_weights()
        if q == 3:
            mixer_step(1)
        if 0 < q and q + 1 < PARTS:
            forward_near(q + 1)
            forward_far(q + 1)
        both_parts = gw.at[:, pl.ds(0, 2 * part_slice(q)[1]), :]
        pltpu.make_async_copy(both_parts, both_parts, expert_sem.at[q]).wait()
        forwarded(q)
        project(q)
        if q == 0:
            forward_near(1)
            forward_far(1)
    pltpu.make_async_copy(dw, dw, down_sem).wait()

    chunk_unit = width // sum(CHUNKS)

    def chunk_cols(j):
        return slice(sum(CHUNKS[:j]) * chunk_unit, sum(CHUNKS[: j + 1]) * chunk_unit)

    def core_rows(c):
        return pl.ds(pl.multiple_of(c * span, span), span)

    y_copies = {}

    def stage_a(j):
        cols = chunk_cols(j)
        size = cols.stop - cols.start
        both_y[:, 0:size] = jnp.dot(hid[...], dw[:, cols], preferred_element_type=F32)
        y_out[:, cols] = both_y[core_rows(c_no), 0:size].astype(BF16)
        y_keep[:, cols] = both_y[core_rows(c_me), 0:size]
        y_copies[j] = remote(
            y_out.at[:, cols], y_in.at[:, cols], yp_s, yp_r.at[j], e_me, partner
        )
        y_copies[j].start()

    def e_rows(e):
        return pl.ds(pl.multiple_of(e * half, half), half)

    def stage_b(j):
        cols = chunk_cols(j)
        y_copies[j].wait_recv()
        y_in[:, cols] = (y_keep[:, cols] + y_in[:, cols].astype(F32)).astype(BF16)
        for e in ep_peers:
            start(
                remote(
                    y_in.at[e_rows(e), cols], e_in.at[e_rows(e_me), cols],
                    ye_s, ye_r.at[j], e, t_me,
                )
            )
        e_in[e_rows(e_me), cols] = y_in[e_rows(e_me), cols]

    def direct(j):
        return j >= len(CHUNKS) - DIRECT

    def stage_c(j):
        cols = chunk_cols(j)
        size = cols.stop - cols.start
        here = e_in.at[pl.ds(0, (ep - 1) * half), pl.ds(0, size)]
        remote(here, here, ye_s, ye_r.at[j], e_me, partner).wait_recv()
        own = parity_rows(spread, c_me, share, core_rows(c_me))
        total = jnp.dot(own, e_in[:, cols], preferred_element_type=F32)
        s_out[:, cols] = total.astype(BF16)
        if direct(j):
            for z in z_peers:
                start(
                    remote(
                        s_out.at[z_rows(z, share), cols], s_in.at[z_me, :, cols],
                        yz_s, yz_r.at[j, 0], e_me, z * CORES + c_me,
                    )
                )
        else:
            z_send(0, s_out, s_in, share, cols, yz_s, yz_r.at[j, 0])
        s_keep[:, cols] = total

    def stage_z(j, s):
        if direct(j):
            return
        cols = chunk_cols(j)
        z_landed(zs >> s, s_in, cols.stop - cols.start, yz_r.at[j, s - 1])
        for m, owner in enumerate(z_owners(z_me, s - 1)):
            rows = z_rows(owner, share)
            total = s_keep[rows, cols] + s_in[z_slot(s - 1) + m, :, cols].astype(F32)
            s_keep[rows, cols] = total
            s_out[rows, cols] = total.astype(BF16)
        z_send(s, s_out, s_in, share, cols, yz_s, yz_r.at[j, s])

    def stage_d(j):
        cols = chunk_cols(j)
        size = cols.stop - cols.start
        total = s_keep[z_rows(z_me, share), cols]
        if direct(j):
            z_landed(zs - 1, s_in, size, yz_r.at[j, 0])
            for z in z_peers:
                total = total + s_in[z, :, cols].astype(F32)
        else:
            z_landed(1, s_in, size, yz_r.at[j, steps - 1])
            total = total + s_in[z_slot(steps - 1), :, cols].astype(F32)
        expert_out[:, cols] = total.astype(BF16)

    def mixer_final():
        z_landed(1, zin, width, mz_r.at[steps - 1])
        total = keep[z_rows(z_me, mix_share), :] + zin[z_slot(steps - 1)].astype(F32)
        mixer_out[...] = total.astype(BF16)

    lag_b, lag_c, lag_z, lag_d = LAGS
    chunks = len(CHUNKS)
    stages = [(stage_a, 0), (stage_b, lag_b), (stage_c, lag_c)]
    for s in range(1, steps):
        stages.append((functools.partial(stage_z, s=s), lag_c + s * lag_z))
    last = lag_c + (steps - 1) * lag_z + lag_d
    stages.append((stage_d, last))
    for step in range(chunks + last):
        for stage, lag in stages:
            if 0 <= step - lag < chunks:
                stage(step - lag)
        if step == 4:
            for s in range(2, steps):
                mixer_step(s)
        if step == chunks:
            mixer_final()

    everything_sent = [
        (pack.at[pl.ds(0, len(near) * half), :], near_s),
        (pack.at[pl.ds(0, len(far) * half), pl.ds(0, width // 2)], far_s),
        (pack.at[pl.ds(0, len(far) * half), pl.ds(0, width // 2)], rel_s),
        (pack.at[pl.ds(0, (ep - 1) * half), :], fwd_s),
        (wpack.at[pl.ds(0, ep - 1)], w_s),
        (pair_out, mp_s),
        (zin.at[pl.ds(0, zs - 1)], mz_s),
        (y_out, yp_s),
        (y_in.at[pl.ds(0, (ep - 1) * half), :], ye_s),
        (s_in.at[pl.ds(0, zs - 1)], yz_s),
    ]
    for ref, sem in everything_sent:
        remote(ref, ref, sem, sem, e_me, partner).wait_send()


def store(a, b, a_out, b_out, sem):
    copies = [pltpu.make_async_copy(s, d, sem.at[i]) for i, (s, d) in enumerate(((a, a_out), (b, b_out)))]
    for c in copies:
        c.start()
    for c in copies:
        c.wait()


def local(ep, tp, *args):
    (mix_tokens, mix_gain, value_w, inner_w, outer_w, taps, mix_w, moe_tokens, moe_gain,
     router_group, router_expert, routes, gate_w, up_w, down_w) = args
    rows, width = mix_tokens.shape
    count = moe_tokens.shape[0]
    channels, hidden = value_w.shape[1], gate_w.shape[2]
    experts_here = gate_w.shape[0]
    zs = tp // CORES
    side = max(s for s in range(1, ep + 1) if ep % s == 0 and s * s <= ep)
    share, mix_share = count // tp, rows // tp
    topk = routes.shape[1]
    slots = experts_here * CAP
    if experts_here % EPG == 0:
        slots = slots // topk
    slots = min(slots, share)
    half = zs * slots
    span = ep * half
    w_rows, w_cols = -(-(experts_here + 1) // 8) * 8, -(-CORES * half // 128) * 128
    chunks = len(CHUNKS)
    chunk = width // sum(CHUNKS) * max(CHUNKS)
    any_ref = pl.BlockSpec(memory_space=pl.ANY)
    vmem = pl.BlockSpec(memory_space=pltpu.VMEM)
    V, D = pltpu.VMEM, lambda *s: pltpu.SemaphoreType.DMA(s)
    one, steps = pltpu.SemaphoreType.DMA, zs.bit_length() - 1
    scratch = [
        V((1, width), F32), V(taps.shape, F32), V((1, width), F32), V(routes.T.shape, jnp.int32),
        V((rows, width), BF16), V((count, width), BF16),
        V(router_group.T.shape, BF16), V(router_expert.T.shape, BF16),
        V(value_w.shape, BF16), V(inner_w.shape, BF16), V(outer_w.shape, BF16),
        V(mix_w.shape, BF16),
        V(gate_w.shape, BF16), V(up_w.shape, BF16), V((experts_here * hidden, width), BF16),
        V((rows, width), BF16), V((count, width), BF16), V((count, 2 * span), BF16), V((2 * span, count), BF16),
        V((2 * span, width), BF16), V((2 * span, width), BF16),
        V((ep, w_rows, w_cols), F32), V((ep, w_rows, w_cols), F32), V((2 * span, w_rows), F32),
        V((rows, channels), BF16), V((16, channels), BF16), V((rows + 8, channels), F32),
        V((rows, channels), BF16), V((rows, channels), BF16),
        V((zs * mix_share, width), BF16), V((zs * mix_share, width), BF16),
        V((zs * mix_share, width), F32),
        V((zs, mix_share, width), BF16),
        V((experts_here, 2 * span, hidden), F32), V((experts_here, 2 * span, hidden), F32),
        V((2 * span, experts_here * hidden), BF16), V((2 * span, chunk), F32),
        V((span, width), BF16), V((span, width), BF16), V((span, width), F32),
        V((span, width), BF16),
        V((zs * share, width), F32), V((zs * share, width), BF16), V((zs, share, width), BF16),
        D(12), D(PARTS), one,
        one, D(PARTS), one, D(PARTS), one, D(PARTS), one, one, one, D(PARTS), one, one,
        one, one, one, D(steps), one, D(chunks), one, D(chunks), one, D(chunks, steps),
    ]
    out = [
        pltpu.VMEM((mix_share, width), BF16),
        pltpu.VMEM((share, width), BF16),
    ]
    in_specs = [any_ref] * len(args)
    results = pl.pallas_call(
        functools.partial(kernel, (ep, side, tp, zs, half, experts_here, w_rows)),
        out_shape=out,
        in_specs=in_specs,
        out_specs=[vmem, vmem],
        scratch_shapes=scratch,
        compiler_params=pltpu.CompilerParams(
            collective_id=0, has_side_effects=True, vmem_limit_bytes=65 * 1024 * 1000
        ),
        name="mixer_and_experts",
    )(
        mix_tokens, mix_gain.reshape(1, width), value_w, inner_w, outer_w, taps, mix_w,
        moe_tokens, moe_gain.reshape(1, width), router_group.T, router_expert.T, routes.T,
        gate_w, up_w, down_w,
    )
    return pl.pallas_call(
        store,
        out_shape=[jax.ShapeDtypeStruct(o.shape, BF16) for o in out],
        in_specs=[vmem, vmem],
        out_specs=[any_ref, any_ref],
        scratch_shapes=[D(2)],
        name="store",
    )(*[pltpu.with_memory_space_constraint(r, pltpu.VMEM) for r in results])


def solution(mesh):
    return jax.shard_map(
        lambda *args: tuple(local(mesh.shape["ep"], mesh.shape["tp"], *args)),
        mesh=mesh,
        in_specs=(
            P("ep", None), P(), P(None, "tp"), P(None, "tp"), P(None, "tp"), P(None, "tp"),
            P("tp", None), P("ep", None), P(), P(), P(), P("ep", None),
            P("ep", None, "tp"), P("ep", None, "tp"), P("ep", "tp", None),
        ),
        out_specs=(P(("ep", "tp"), None), P(("ep", "tp"), None)),
        check_vma=False,
    )
```

```python
import functools

import jax
import jax.numpy as jnp
from jax import lax
from jax.experimental import pallas as pl
from jax.experimental.pallas import tpu as pltpu
from jax.sharding import PartitionSpec as P

EPG = 4
CAP = 4
CORES = 2
CHUNKS = (1, 2, 2, 2, 2, 2, 2, 1, 1, 1)
LAGS = (1,6,2,10)
DIRECT = 10
SPLIT = (2, 2, 2, 2)
PARTS = len(SPLIT)
HOOK = 0
MESH = pl.DeviceIdType.MESH
F32, BF16 = jnp.float32, jnp.bfloat16


def iota(shape, dim):
    return lax.broadcasted_iota(jnp.int32, shape, dim)


def norm_rows(src, gain, dst):
    width = src.shape[1]

    def body(i, carry):
        rows = pl.ds(pl.multiple_of(i * 16, 16), 16)
        x = src[rows, :].astype(F32)
        inv = lax.rsqrt(jnp.sum(x * x, axis=1, keepdims=True) * (1.0 / width) + 1e-06)
        dst[rows, :] = (x * inv * gain[...]).astype(BF16)
        return carry

    lax.fori_loop(0, src.shape[0] // 16, body, 0, unroll=4)


def row_scales(src):
    width = src.shape[1]
    total = None
    for first in range(0, width, 512):
        x = src[:, first : first + 512].astype(F32)
        square = x * x
        total = square if total is None else total + square
    return lax.rsqrt(jnp.sum(total, axis=1, keepdims=True) * (1.0 / width) + 1e-06)


def column_tiles(first, last, tile, body):
    def step(i, carry):
        body(pl.ds(pl.multiple_of(i * tile, tile), tile))
        return carry

    lax.fori_loop(first // tile, last // tile, step, 0, unroll=4)


def kernel(
    cfg,
    mix_tokens, mix_gain_in, value_w, inner_w, outer_w, taps_in, mix_w, moe_tokens, moe_gain_in,
    router_group, router_expert, routes_in, gate_w, up_w, down_w,
    mixer_out, expert_out,
    mix_gain, taps, moe_gain, routes, xm, xe, rg, rx, vw, iw, ow, mw, gw, uw, dw,
    nm, ne, spread, gather, pack, got, wpack, wgot, wrow,
    gated, halo, padded, conv, ordered, pair_out, pair_in, keep, zin,
    gate_acc, up_acc, hid, both_y, y_out, y_in, y_keep, e_in, s_keep, s_out, s_in,
    load_sem, expert_sem, down_sem,
    near_s, near_r, far_s, far_r, rel_s, rel_r, w_s, w_r, fwd_s, fwd_r, halo_s, halo_r,
    mp_s, mp_r, mz_s, mz_r, yp_s, yp_r, ye_s, ye_r, yz_s, yz_r,
):
    ep, side, tp, zs, half, experts_here, w_rows = cfg
    e_me, t_me = lax.axis_index("ep"), lax.axis_index("tp")
    z_me, c_me = t_me // CORES, lax.rem(t_me, CORES)
    c_no = 1 - c_me
    partner = z_me * CORES + c_no
    width = xm.shape[1]
    tall = ep // side
    e_row, e_col = e_me // side, lax.rem(e_me, side)

    def placed(down, across):
        return lax.rem(e_row + down, tall) * side + lax.rem(e_col + across, side)

    near = [placed(d, 0) for d in range(1, tall)] + [placed(0, a) for a in range(1, side)]
    far = [placed(d, a) for d in range(1, tall) for a in range(1, side)]
    ep_peers = near + far
    z_odd = lax.rem(z_me, 2)
    z_pair = z_me + 1 - 2 * z_odd
    z_peers = [lax.rem(z_me + d, zs) for d in range(1, zs)]

    def start(copy):
        copy.start()

    barrier = pltpu.get_barrier_semaphore()
    for e in ep_peers:
        pl.semaphore_signal(barrier, inc=1, device_id={"ep": e, "tp": t_me}, device_id_type=MESH)
    for z in z_peers:
        pl.semaphore_signal(
            barrier, inc=1, device_id={"ep": e_me, "tp": z * CORES + c_me}, device_id_type=MESH
        )
    pl.semaphore_signal(barrier, inc=1, device_id={"ep": e_me, "tp": partner}, device_id_type=MESH)

    def load(k, src, dst):
        return pltpu.make_async_copy(src, dst, load_sem.at[k])

    loads = [
        load(k, s, d)
        for k, (s, d) in enumerate(
            [
                (moe_tokens, xe), (router_group, rg), (router_expert, rx), (mix_tokens, xm),
                (value_w, vw), (inner_w, iw), (outer_w, ow), (mix_w, mw),
                (routes_in, routes), (moe_gain_in, moe_gain), (mix_gain_in, mix_gain), (taps_in, taps),
            ]
        )
    ]
    unit = width // sum(SPLIT)

    def part_slice(q):
        return sum(SPLIT[:q]) * unit, SPLIT[q] * unit

    def expert_loads(q):
        rows = pl.ds(*part_slice(q))
        return [
            pltpu.make_async_copy(gate_w.at[:, rows, :], gw.at[:, rows, :], expert_sem.at[q]),
            pltpu.make_async_copy(up_w.at[:, rows, :], uw.at[:, rows, :], expert_sem.at[q]),
        ]

    hidden = down_w.shape[1]
    down_loads = [
        pltpu.make_async_copy(
            down_w.at[k], dw.at[k * hidden : (k + 1) * hidden, :], down_sem
        )
        for k in range(experts_here)
    ]
    for k in (8, 0, 9, 3, 10, 4, 5):
        loads[k].start()

    def remote(src, dst, s_sem, r_sem, e, t):
        return pltpu.make_async_remote_copy(
            src_ref=src, dst_ref=dst, send_sem=s_sem, recv_sem=r_sem,
            device_id={"ep": e, "tp": t}, device_id_type=MESH,
        )

    count = xe.shape[0]
    share = count // tp
    slots = half // zs
    span = ep * half
    loads[8].wait()
    diagonal = jnp.where(iota((count, count), 0) == iota((count, count), 1), 1.0, 0.0)
    r = lax.dot_general(
        diagonal.astype(BF16), routes[...].astype(F32).astype(BF16), (((1,), (1,)), ((), ())),
        preferred_element_type=F32,
    ).astype(jnp.int32)
    picks = [r[:, 0:1], r[:, 1:2]]
    lane = iota((count, -(-ep * w_rows // 128) * 128), 1)
    shards = [
        sum((p >= s * experts_here).astype(jnp.int32) for s in range(1, ep)) for p in picks
    ]
    member = jnp.where((lane == shards[0]) | (lane == shards[1]), 1.0, 0.0).astype(BF16)
    ti, tj = iota((count, count), 0), iota((count, count), 1)
    earlier = jnp.where(((ti ^ tj) < share) & (tj < ti), 1.0, 0.0).astype(BF16)
    rank = jnp.dot(earlier, member, preferred_element_type=F32)
    block = lax.shift_right_logical(iota((count, 1), 0), share.bit_length() - 1)
    base = (block & 1) * span + lax.shift_right_logical(block, 1) * slots
    slot_lane = iota((count, 2 * span), 1)
    hits = []
    for s in shards:
        mine = jnp.sum(jnp.where(lane == s, rank, 0.0), axis=1, keepdims=True).astype(jnp.int32)
        hits.append(slot_lane == base + s * half + mine)
    one_hot = jnp.where(hits[0] | hits[1], 1.0, 0.0).astype(BF16)
    spread[...] = one_hot
    gather[...] = lax.dot_general(
        one_hot, diagonal.astype(BF16), (((0,), (0,)), ((), ())), preferred_element_type=F32
    ).astype(BF16)
    loads[0].wait()
    loads[9].wait()

    def pack_part(q):
        first, size = part_slice(q)
        cols = slice(first, first + size)
        ne[:, cols] = (xe[:, cols].astype(F32) * moe_gain[:, cols]).astype(BF16)
        pack[:, cols] = jnp.dot(
            gather[...], ne[:, cols], preferred_element_type=F32
        ).astype(BF16)

    pack_part(0)
    pack_part(1)
    for k in (1, 2, 6, 11, 7):
        loads[k].start()
    for c in expert_loads(0):
        c.start()
    pl.semaphore_wait(barrier, (ep - 1) + (zs - 1) + 1)
    def half_rows(c, e):
        return pl.ds(pl.multiple_of(c * span + e * half, half), half)

    def half_cols(q, odd):
        first, size = part_slice(q)
        return pl.ds(pl.multiple_of(first + odd * (size // 2), 128), size // 2)

    def dispatch(q, peers, cols, s_sem, r_sem):
        for e in peers:
            start(
                remote(
                    pack.at[half_rows(c_me, e), cols], got.at[half_rows(c_me, e_me), cols],
                    s_sem, r_sem.at[q], e, t_me,
                )
            )

    def dispatch_far(q):
        dispatch(q, far, half_cols(q, z_odd), far_s, far_r)

    def dispatch_near(q):
        dispatch(q, near, pl.ds(*part_slice(q)), near_s, near_r)

    def landed(count, size, sem):
        here = got.at[pl.ds(0, count * half), pl.ds(0, size)]
        remote(here, here, sem, sem, e_me, partner).wait_recv()

    def forward(q, e, cols):
        here = got.at[half_rows(c_me, e), cols]
        start(remote(here, here, fwd_s, fwd_r.at[q], e_me, partner))

    def relay(q):
        cols = half_cols(q, z_odd)
        landed(len(far), part_slice(q)[1] // 2, far_r.at[q])
        for e in far:
            here = got.at[half_rows(c_me, e), cols]
            start(remote(here, here, rel_s, rel_r.at[q], e_me, z_pair * CORES + c_me))
            forward(q, e, cols)

    def forward_near(q):
        landed(len(near), part_slice(q)[1], near_r.at[q])
        for e in near:
            forward(q, e, pl.ds(*part_slice(q)))

    def forward_far(q):
        landed(len(far), part_slice(q)[1] // 2, rel_r.at[q])
        for e in far:
            forward(q, e, half_cols(q, 1 - z_odd))

    def forwarded(q):
        landed(ep - 1, part_slice(q)[1], fwd_r.at[q])

    dispatch_far(0)
    dispatch_far(1)
    for q in range(2, PARTS):
        pack_part(q)
        dispatch_far(q)
    loads[3].wait()
    loads[10].wait()
    norm_rows(xm, mix_gain, nm)
    loads[4].wait()
    loads[5].wait()
    rows = xm.shape[0]
    value_proj = jnp.dot(nm[...], vw[...], preferred_element_type=F32)
    inner_proj = jnp.dot(nm[...], iw[...], preferred_element_type=F32)
    gated[...] = (inner_proj * value_proj).astype(BF16)
    halo_copy = remote(
        gated.at[pl.ds(rows - 16, 16), :], halo, halo_s, halo_r,
        lax.rem(e_me + 1, ep), t_me,
    )
    halo_copy.start()
    for q in range(PARTS - 1):
        dispatch_near(q)
    for q in range(1, PARTS):
        for c in expert_loads(q):
            c.start()
    loads[1].wait()
    loads[2].wait()
    lanes = (((1,), (1,)), ((), ()))
    row_scale = row_scales(xe)
    group_exp = jnp.exp(
        row_scale * lax.dot_general(ne[...], rg[...], lanes, preferred_element_type=F32)
    )
    expert_logit = row_scale * lax.dot_general(
        ne[...], rx[...], lanes, preferred_element_type=F32
    )
    groups, experts = group_exp.shape[1], expert_logit.shape[1]
    group = sum((picks[0] >= s * EPG).astype(jnp.int32) for s in range(1, groups))
    chosen_group = jnp.where(iota((count, groups), 1) == group, group_exp, 0.0)
    group_gate = jnp.sum(chosen_group, axis=1, keepdims=True) / jnp.sum(
        group_exp, axis=1, keepdims=True
    )
    expert_lane = iota((count, experts), 1)
    chosen = [
        jnp.exp(jnp.sum(jnp.where(expert_lane == p, expert_logit, 0.0), axis=1, keepdims=True))
        for p in picks
    ]
    scale = chosen[0] + chosen[1]
    w_lanes = [s * w_rows + (p - s * experts_here) for s, p in zip(shards, picks)]
    weights = sum(
        jnp.where(lane == at, group_gate * c / scale, 0.0) for at, c in zip(w_lanes, chosen)
    )
    scale_lanes = [s * w_rows + experts_here for s in shards]
    weights = weights + jnp.where(
        (lane == scale_lanes[0]) | (lane == scale_lanes[1]), row_scale, 0.0
    )

    def three_parts(value):
        parts = []
        for _ in range(3):
            parts.append(value.astype(BF16))
            value = value - parts[-1].astype(F32)
        return parts

    packed_w = sum(
        lax.dot_general(p, spread[...], (((0,), (0,)), ((), ())), preferred_element_type=F32)
        for p in three_parts(weights)
    )
    for e in range(ep):
        for c in range(CORES):
            wpack[e, :, c * half : (c + 1) * half] = packed_w[
                e * w_rows : (e + 1) * w_rows, c * span + e * half : c * span + (e + 1) * half
            ]
    wgot[e_me] = wpack[e_me]
    for c in range(CORES):
        got[half_rows(c, e_me), :] = pack[half_rows(c, e_me), :]

    for e in ep_peers:
        start(remote(wpack.at[e], wgot.at[e_me], w_s, w_r, e, t_me))
    dispatch_near(PARTS - 1)
    padded[8:, :] = gated[...].astype(F32)
    loads[6].wait()
    outer_proj = jnp.dot(nm[...], ow[...], preferred_element_type=F32)
    mix_share = rows // tp
    mix_rows = zs * mix_share
    everything = slice(None)
    pair_copy = remote(pair_out, pair_in, mp_s, mp_r, e_me, partner)

    def parity_rows(ref, c, step, cols):
        return jnp.concatenate(
            [
                ref[pl.ds(pl.multiple_of((z * CORES + c) * step, step), step), cols]
                for z in range(zs)
            ],
            axis=0,
        )

    def z_rows(z, step):
        return pl.ds(pl.multiple_of(z * step, step), step)

    steps = zs.bit_length() - 1

    def z_partner(s):
        return z_me + (1 - 2 * lax.rem(z_me // 2**s, 2)) * 2**s

    def z_owners(z, s):
        low = lax.rem(z, 2 ** (s + 1))
        return [low + m * 2 ** (s + 1) for m in range(zs >> (s + 1))]

    def z_slot(s):
        return sum(zs >> (t + 1) for t in range(s))

    def z_send(s, src, dst, step, cols, s_sem, r_sem):
        to = z_partner(s)
        for m, owner in enumerate(z_owners(to, s)):
            start(
                remote(
                    src.at[z_rows(owner, step), cols], dst.at[z_slot(s) + m, :, cols],
                    s_sem, r_sem, e_me, to * CORES + c_me,
                )
            )

    def z_landed(blocks, ref, size, sem):
        here = ref.at[pl.ds(0, blocks), :, pl.ds(0, size)]
        remote(here, here, sem, sem, e_me, partner).wait_recv()

    def mixer_pair():
        halo_copy.wait()
        before = halo[...].astype(F32)[8:16, :]
        padded[0:8, :] = jnp.where(e_me > 0, before, jnp.zeros_like(before))
        loads[11].wait()
        n_taps = taps.shape[0]
        mixed = taps[0:1, :] * padded[pl.ds(9 - n_taps, rows), :]
        for j in range(1, n_taps):
            mixed = mixed + taps[j : j + 1, :] * padded[pl.ds(9 - n_taps + j, rows), :]
        conv[...] = (outer_proj * mixed).astype(BF16)

        loads[7].wait()

        ordered[0:mix_rows, :] = parity_rows(conv, c_no, mix_share, everything)
        ordered[mix_rows:, :] = parity_rows(conv, c_me, mix_share, everything)

        def mix_tile(cols):
            both = jnp.dot(ordered[...], mw[:, cols], preferred_element_type=F32)
            pair_out[:, cols] = both[0:mix_rows].astype(BF16)
            keep[:, cols] = both[mix_rows:]

        column_tiles(0, width // 2, 512, mix_tile)
        forward_near(0)
        forward_far(0)
        column_tiles(width // 2, width, 512, mix_tile)
        pair_copy.start()

    def mixer_sums():
        pair_copy.wait_recv()

        def sum_tile(cols):
            total = keep[:, cols] + pair_in[:, cols].astype(F32)
            keep[:, cols] = total
            pair_in[:, cols] = total.astype(BF16)

        column_tiles(0, width, 512, sum_tile)

        for z in z_peers:
            start(
                remote(
                    pair_in.at[z_rows(z, mix_share), :], zin.at[z_me], mz_s, mz_r,
                    e_me, z * CORES + c_me,
                )
            )

    def project(q):
        first, size = part_slice(q)
        cols = slice(first, first + size)

        for k in range(experts_here):
            if k == HOOK and q + 1 < PARTS:
                forward_near(q + 1)
                forward_far(q + 1)
            gate = jnp.dot(got[:, cols], gw[k, cols, :], preferred_element_type=F32)
            up = jnp.dot(got[:, cols], uw[k, cols, :], preferred_element_type=F32)
            if q:
                gate = gate + gate_acc[k]
                up = up + up_acc[k]
            if q < PARTS - 1:
                gate_acc[k] = gate
                up_acc[k] = up
                continue
            row = wrow[:, experts_here : experts_here + 1]
            gate = gate * row
            hid[:, k * hidden : (k + 1) * hidden] = (gate / (1.0 + jnp.exp(-gate)) * up * (row * wrow[:, k : k + 1])).astype(BF16)

    def arrived_weights():
        arrived = wgot.at[pl.ds(0, ep - 1)]
        remote(arrived, arrived, w_s, w_r, e_me, partner).wait_recv()
        across = jnp.concatenate(
            [wgot[e, :, c * half : (c + 1) * half] for c in range(CORES) for e in range(ep)], axis=1
        )
        square = (2 * span, 2 * span)
        same = jnp.where(iota(square, 0) == iota(square, 1), 1.0, 0.0).astype(BF16)
        wrow[...] = sum(
            lax.dot_general(same, p, lanes, preferred_element_type=F32)
            for p in three_parts(across)
        )

    for c in down_loads:
        c.start()
    for q in range(PARTS):
        relay(q)
    mixer_pair()
    for q in range(PARTS):
        if q == 1:
            mixer_sums()
        if q == PARTS - 1:
            arrived_weights()
        both_parts = gw.at[:, pl.ds(0, 2 * part_slice(q)[1]), :]
        pltpu.make_async_copy(both_parts, both_parts, expert_sem.at[q]).wait()
        forwarded(q)
        project(q)
    pltpu.make_async_copy(dw, dw, down_sem).wait()

    chunk_unit = width // sum(CHUNKS)

    def chunk_cols(j):
        return slice(sum(CHUNKS[:j]) * chunk_unit, sum(CHUNKS[: j + 1]) * chunk_unit)

    def core_rows(c):
        return pl.ds(pl.multiple_of(c * span, span), span)

    y_copies = {}

    def stage_a(j):
        cols = chunk_cols(j)
        size = cols.stop - cols.start
        both_y[:, 0:size] = jnp.dot(hid[...], dw[:, cols], preferred_element_type=F32)
        y_out[:, cols] = both_y[core_rows(c_no), 0:size].astype(BF16)
        y_keep[:, cols] = both_y[core_rows(c_me), 0:size]
        y_copies[j] = remote(
            y_out.at[:, cols], y_in.at[:, cols], yp_s, yp_r.at[j], e_me, partner
        )
        y_copies[j].start()

    def e_rows(e):
        return pl.ds(pl.multiple_of(e * half, half), half)

    def stage_b(j):
        cols = chunk_cols(j)
        y_copies[j].wait_recv()
        y_in[:, cols] = (y_keep[:, cols] + y_in[:, cols].astype(F32)).astype(BF16)
        for e in ep_peers:
            start(
                remote(
                    y_in.at[e_rows(e), cols], e_in.at[e_rows(e_me), cols],
                    ye_s, ye_r.at[j], e, t_me,
                )
            )
        e_in[e_rows(e_me), cols] = y_in[e_rows(e_me), cols]

    def direct(j):
        return j >= len(CHUNKS) - DIRECT

    def stage_c(j):
        cols = chunk_cols(j)
        size = cols.stop - cols.start
        here = e_in.at[pl.ds(0, (ep - 1) * half), pl.ds(0, size)]
        remote(here, here, ye_s, ye_r.at[j], e_me, partner).wait_recv()
        own = parity_rows(spread, c_me, share, core_rows(c_me))
        total = jnp.dot(own, e_in[:, cols], preferred_element_type=F32)
        s_out[:, cols] = total.astype(BF16)
        if direct(j):
            for z in z_peers:
                start(
                    remote(
                        s_out.at[z_rows(z, share), cols], s_in.at[z_me, :, cols],
                        yz_s, yz_r.at[j, 0], e_me, z * CORES + c_me,
                    )
                )
        else:
            z_send(0, s_out, s_in, share, cols, yz_s, yz_r.at[j, 0])
        s_keep[:, cols] = total

    def stage_z(j, s):
        if direct(j):
            return
        cols = chunk_cols(j)
        z_landed(zs >> s, s_in, cols.stop - cols.start, yz_r.at[j, s - 1])
        for m, owner in enumerate(z_owners(z_me, s - 1)):
            rows = z_rows(owner, share)
            total = s_keep[rows, cols] + s_in[z_slot(s - 1) + m, :, cols].astype(F32)
            s_keep[rows, cols] = total
            s_out[rows, cols] = total.astype(BF16)
        z_send(s, s_out, s_in, share, cols, yz_s, yz_r.at[j, s])

    def stage_d(j):
        cols = chunk_cols(j)
        size = cols.stop - cols.start
        total = s_keep[z_rows(z_me, share), cols]
        if direct(j):
            z_landed(zs - 1, s_in, size, yz_r.at[j, 0])
            for z in z_peers:
                total = total + s_in[z, :, cols].astype(F32)
        else:
            z_landed(1, s_in, size, yz_r.at[j, steps - 1])
            total = total + s_in[z_slot(steps - 1), :, cols].astype(F32)
        expert_out[:, cols] = total.astype(BF16)

    def mixer_final():
        z_landed(zs - 1, zin, width, mz_r)
        total = keep[z_rows(z_me, mix_share), :]
        for z in z_peers:
            total = total + zin[z].astype(F32)
        mixer_out[...] = total.astype(BF16)

    lag_b, lag_c, lag_z, lag_d = LAGS
    chunks = len(CHUNKS)
    stages = [(stage_a, 0), (stage_b, lag_b), (stage_c, lag_c)]
    for s in range(1, steps):
        stages.append((functools.partial(stage_z, s=s), lag_c + s * lag_z))
    last = lag_c + (steps - 1) * lag_z + lag_d
    stages.append((stage_d, last))
    for step in range(chunks + last):
        for stage, lag in stages:
            if 0 <= step - lag < chunks:
                stage(step - lag)
        if step == chunks + lag_c - 1:
            mixer_final()

    everything_sent = [
        (pack.at[pl.ds(0, len(near) * half), :], near_s),
        (pack.at[pl.ds(0, len(far) * half), pl.ds(0, width // 2)], far_s),
        (pack.at[pl.ds(0, len(far) * half), pl.ds(0, width // 2)], rel_s),
        (pack.at[pl.ds(0, (ep - 1) * half), :], fwd_s),
        (wpack.at[pl.ds(0, ep - 1)], w_s),
        (pair_out, mp_s),
        (zin.at[pl.ds(0, zs - 1)], mz_s),
        (y_out, yp_s),
        (y_in.at[pl.ds(0, (ep - 1) * half), :], ye_s),
        (s_in.at[pl.ds(0, zs - 1)], yz_s),
    ]
    for ref, sem in everything_sent:
        remote(ref, ref, sem, sem, e_me, partner).wait_send()


def store(a, b, a_out, b_out, sem):
    copies = [pltpu.make_async_copy(s, d, sem.at[i]) for i, (s, d) in enumerate(((a, a_out), (b, b_out)))]
    for c in copies:
        c.start()
    for c in copies:
        c.wait()


def local(ep, tp, *args):
    (mix_tokens, mix_gain, value_w, inner_w, outer_w, taps, mix_w, moe_tokens, moe_gain,
     router_group, router_expert, routes, gate_w, up_w, down_w) = args
    rows, width = mix_tokens.shape
    count = moe_tokens.shape[0]
    channels, hidden = value_w.shape[1], gate_w.shape[2]
    experts_here = gate_w.shape[0]
    zs = tp // CORES
    side = max(s for s in range(1, ep + 1) if ep % s == 0 and s * s <= ep)
    share, mix_share = count // tp, rows // tp
    topk = routes.shape[1]
    slots = experts_here * CAP
    if experts_here % EPG == 0:
        slots = slots // topk
    slots = min(slots, share)
    half = zs * slots
    span = ep * half
    w_rows, w_cols = -(-(experts_here + 1) // 8) * 8, -(-CORES * half // 128) * 128
    chunks = len(CHUNKS)
    chunk = width // sum(CHUNKS) * max(CHUNKS)
    any_ref = pl.BlockSpec(memory_space=pl.ANY)
    vmem = pl.BlockSpec(memory_space=pltpu.VMEM)
    V, D = pltpu.VMEM, lambda *s: pltpu.SemaphoreType.DMA(s)
    one, steps = pltpu.SemaphoreType.DMA, zs.bit_length() - 1
    scratch = [
        V((1, width), F32), V(taps.shape, F32), V((1, width), F32), V(routes.T.shape, jnp.int32),
        V((rows, width), BF16), V((count, width), BF16),
        V(router_group.T.shape, BF16), V(router_expert.T.shape, BF16),
        V(value_w.shape, BF16), V(inner_w.shape, BF16), V(outer_w.shape, BF16),
        V(mix_w.shape, BF16),
        V(gate_w.shape, BF16), V(up_w.shape, BF16), V((experts_here * hidden, width), BF16),
        V((rows, width), BF16), V((count, width), BF16), V((count, 2 * span), BF16), V((2 * span, count), BF16),
        V((2 * span, width), BF16), V((2 * span, width), BF16),
        V((ep, w_rows, w_cols), F32), V((ep, w_rows, w_cols), F32), V((2 * span, w_rows), F32),
        V((rows, channels), BF16), V((16, channels), BF16), V((rows + 8, channels), F32),
        V((rows, channels), BF16), V((rows, channels), BF16),
        V((zs * mix_share, width), BF16), V((zs * mix_share, width), BF16),
        V((zs * mix_share, width), F32),
        V((zs, mix_share, width), BF16),
        V((experts_here, 2 * span, hidden), F32), V((experts_here, 2 * span, hidden), F32),
        V((2 * span, experts_here * hidden), BF16), V((2 * span, chunk), F32),
        V((span, width), BF16), V((span, width), BF16), V((span, width), F32),
        V((span, width), BF16),
        V((zs * share, width), F32), V((zs * share, width), BF16), V((zs, share, width), BF16),
        D(12), D(PARTS), one,
        one, D(PARTS), one, D(PARTS), one, D(PARTS), one, one, one, D(PARTS), one, one,
        one, one, one, one, one, D(chunks), one, D(chunks), one, D(chunks, steps),
    ]
    out = [
        pltpu.VMEM((mix_share, width), BF16),
        pltpu.VMEM((share, width), BF16),
    ]
    in_specs = [any_ref] * len(args)
    results = pl.pallas_call(
        functools.partial(kernel, (ep, side, tp, zs, half, experts_here, w_rows)),
        out_shape=out,
        in_specs=in_specs,
        out_specs=[vmem, vmem],
        scratch_shapes=scratch,
        compiler_params=pltpu.CompilerParams(
            collective_id=0, has_side_effects=True, vmem_limit_bytes=65 * 1024 * 1000
        ),
        name="mixer_and_experts",
    )(
        mix_tokens, mix_gain.reshape(1, width), value_w, inner_w, outer_w, taps, mix_w,
        moe_tokens, moe_gain.reshape(1, width), router_group.T, router_expert.T, routes.T,
        gate_w, up_w, down_w,
    )
    return pl.pallas_call(
        store,
        out_shape=[jax.ShapeDtypeStruct(o.shape, BF16) for o in out],
        in_specs=[vmem, vmem],
        out_specs=[any_ref, any_ref],
        scratch_shapes=[D(2)],
        name="store",
    )(*[pltpu.with_memory_space_constraint(r, pltpu.VMEM) for r in results])


def solution(mesh):
    return jax.shard_map(
        lambda *args: tuple(local(mesh.shape["ep"], mesh.shape["tp"], *args)),
        mesh=mesh,
        in_specs=(
            P("ep", None), P(), P(None, "tp"), P(None, "tp"), P(None, "tp"), P(None, "tp"),
            P("tp", None), P("ep", None), P(), P(), P(), P("ep", None),
            P("ep", None, "tp"), P("ep", None, "tp"), P("ep", "tp", None),
        ),
        out_specs=(P(("ep", "tp"), None), P(("ep", "tp"), None)),
        check_vma=False,
    )
```

```python
import functools

import jax
import jax.numpy as jnp
from jax import lax
from jax.experimental import pallas as pl
from jax.experimental.pallas import tpu as pltpu
from jax.sharding import PartitionSpec as P

EPG = 4
CAP = 4
CORES = 2
CHUNKS = (1, 3, 4, 4, 4, 4, 4, 4, 2, 2)
LAGS = (1, 6)
SPLIT = (2, 2, 2, 2)
PARTS = len(SPLIT)
HOOK = 0
MESH = pl.DeviceIdType.MESH
F32, BF16 = jnp.float32, jnp.bfloat16


def iota(shape, dim):
    return lax.broadcasted_iota(jnp.int32, shape, dim)


def norm_rows(src, gain, dst):
    width = src.shape[1]

    def body(i, carry):
        rows = pl.ds(pl.multiple_of(i * 16, 16), 16)
        x = src[rows, :].astype(F32)
        inv = lax.rsqrt(jnp.sum(x * x, axis=1, keepdims=True) * (1.0 / width) + 1e-06)
        dst[rows, :] = (x * inv * gain[...]).astype(BF16)
        return carry

    lax.fori_loop(0, src.shape[0] // 16, body, 0, unroll=4)


def row_scales(src):
    width = src.shape[1]
    total = None
    for first in range(0, width, 512):
        x = src[:, first : first + 512].astype(F32)
        square = x * x
        total = square if total is None else total + square
    return lax.rsqrt(jnp.sum(total, axis=1, keepdims=True) * (1.0 / width) + 1e-06)


def column_tiles(first, last, tile, body):
    def step(i, carry):
        body(pl.ds(pl.multiple_of(i * tile, tile), tile))
        return carry

    lax.fori_loop(first // tile, last // tile, step, 0, unroll=4)


def kernel(
    cfg,
    mix_tokens, mix_gain_in, value_w, inner_w, outer_w, taps_in, mix_w, moe_tokens, moe_gain_in,
    router_group, router_expert, routes_in, gate_w, up_w, down_w,
    mixer_out, expert_out,
    mix_gain, taps, moe_gain, routes, xm, xe, rg, rx, vw, iw, ow, mw, gw, uw, dw,
    nm, ne, spread, gather, pack, got, wpack, wgot, wrow,
    gated, halo, padded, conv, ordered, pair_out, pair_in, keep, zin,
    gate_acc, up_acc, hid, both_y, y_out, y_in, y_keep, e_in, s_keep, s_out, s_in,
    load_sem, expert_sem, down_sem,
    near_s, near_r, far_s, far_r, rel_s, rel_r, w_s, w_r, fwd_s, fwd_r, halo_s, halo_r,
    mp_s, mp_r, mz_s, mz_r, yp_s, yp_r, ye_s, ye_r, yz_s, yz_r,
):
    ep, side, tp, zs, half, experts_here, w_rows = cfg
    e_me, t_me = lax.axis_index("ep"), lax.axis_index("tp")
    z_me, c_me = t_me // CORES, lax.rem(t_me, CORES)
    c_no = 1 - c_me
    partner = z_me * CORES + c_no
    width = xm.shape[1]
    tall = ep // side
    e_row, e_col = e_me // side, lax.rem(e_me, side)

    def placed(down, across):
        return lax.rem(e_row + down, tall) * side + lax.rem(e_col + across, side)

    near = [placed(d, 0) for d in range(1, tall)] + [placed(0, a) for a in range(1, side)]
    far = [placed(d, a) for d in range(1, tall) for a in range(1, side)]
    ep_peers = near + far
    z_odd = lax.rem(z_me, 2)
    z_pair = z_me + 1 - 2 * z_odd

    def z_flipped(bits):
        z = z_me
        for b in range(zs.bit_length() - 1):
            if bits >> b & 1:
                z = z + (1 - 2 * lax.rem(z_me // 2**b, 2)) * 2**b
        return z

    z_peers = [z_flipped(bits) for bits in range(zs - 1, 0, -1)]

    def start(copy):
        copy.start()

    barrier = pltpu.get_barrier_semaphore()
    for e in ep_peers:
        pl.semaphore_signal(barrier, inc=1, device_id={"ep": e, "tp": t_me}, device_id_type=MESH)
    for z in z_peers:
        pl.semaphore_signal(
            barrier, inc=1, device_id={"ep": e_me, "tp": z * CORES + c_me}, device_id_type=MESH
        )
    pl.semaphore_signal(barrier, inc=1, device_id={"ep": e_me, "tp": partner}, device_id_type=MESH)

    def load(k, src, dst):
        return pltpu.make_async_copy(src, dst, load_sem.at[k])

    loads = [
        load(k, s, d)
        for k, (s, d) in enumerate(
            [
                (moe_tokens, xe), (router_group, rg), (router_expert, rx), (mix_tokens, xm),
                (value_w, vw), (inner_w, iw), (outer_w, ow), (mix_w, mw),
                (routes_in, routes), (moe_gain_in, moe_gain), (mix_gain_in, mix_gain), (taps_in, taps),
            ]
        )
    ]
    unit = width // sum(SPLIT)

    def part_slice(q):
        return sum(SPLIT[:q]) * unit, SPLIT[q] * unit

    def expert_loads(q):
        rows = pl.ds(*part_slice(q))
        return [
            pltpu.make_async_copy(gate_w.at[:, rows, :], gw.at[:, rows, :], expert_sem.at[q]),
            pltpu.make_async_copy(up_w.at[:, rows, :], uw.at[:, rows, :], expert_sem.at[q]),
        ]

    hidden = down_w.shape[1]
    down_loads = [
        pltpu.make_async_copy(
            down_w.at[k], dw.at[k * hidden : (k + 1) * hidden, :], down_sem
        )
        for k in range(experts_here)
    ]
    for k in (8, 0, 9, 3, 10, 4, 5):
        loads[k].start()

    def remote(src, dst, s_sem, r_sem, e, t):
        return pltpu.make_async_remote_copy(
            src_ref=src, dst_ref=dst, send_sem=s_sem, recv_sem=r_sem,
            device_id={"ep": e, "tp": t}, device_id_type=MESH,
        )

    count = xe.shape[0]
    share = count // tp
    slots = half // zs
    span = ep * half
    loads[8].wait()
    diagonal = jnp.where(iota((count, count), 0) == iota((count, count), 1), 1.0, 0.0)
    r = lax.dot_general(
        diagonal.astype(BF16), routes[...].astype(F32).astype(BF16), (((1,), (1,)), ((), ())),
        preferred_element_type=F32,
    ).astype(jnp.int32)
    picks = [r[:, 0:1], r[:, 1:2]]
    lane = iota((count, -(-ep * w_rows // 128) * 128), 1)
    shards = [
        sum((p >= s * experts_here).astype(jnp.int32) for s in range(1, ep)) for p in picks
    ]
    member = jnp.where((lane == shards[0]) | (lane == shards[1]), 1.0, 0.0).astype(BF16)
    ti, tj = iota((count, count), 0), iota((count, count), 1)
    earlier = jnp.where(((ti ^ tj) < share) & (tj < ti), 1.0, 0.0).astype(BF16)
    rank = jnp.dot(earlier, member, preferred_element_type=F32)
    block = lax.shift_right_logical(iota((count, 1), 0), share.bit_length() - 1)
    base = (block & 1) * span + lax.shift_right_logical(block, 1) * slots
    slot_lane = iota((count, 2 * span), 1)
    hits = []
    for s in shards:
        mine = jnp.sum(jnp.where(lane == s, rank, 0.0), axis=1, keepdims=True).astype(jnp.int32)
        hits.append(slot_lane == base + s * half + mine)
    one_hot = jnp.where(hits[0] | hits[1], 1.0, 0.0).astype(BF16)
    spread[...] = one_hot
    gather[...] = lax.dot_general(
        one_hot, diagonal.astype(BF16), (((0,), (0,)), ((), ())), preferred_element_type=F32
    ).astype(BF16)
    loads[0].wait()
    loads[9].wait()

    def pack_part(q):
        first, size = part_slice(q)
        cols = slice(first, first + size)
        ne[:, cols] = (xe[:, cols].astype(F32) * moe_gain[:, cols]).astype(BF16)
        pack[:, cols] = jnp.dot(
            gather[...], ne[:, cols], preferred_element_type=F32
        ).astype(BF16)

    pack_part(0)
    pack_part(1)
    for k in (1, 2, 6, 11, 7):
        loads[k].start()
    for c in expert_loads(0):
        c.start()
    pl.semaphore_wait(barrier, (ep - 1) + (zs - 1) + 1)
    def half_rows(c, e):
        return pl.ds(pl.multiple_of(c * span + e * half, half), half)

    def half_cols(q, odd):
        first, size = part_slice(q)
        return pl.ds(pl.multiple_of(first + odd * (size // 2), 128), size // 2)

    def dispatch(q, peers, cols, s_sem, r_sem):
        for e in peers:
            start(
                remote(
                    pack.at[half_rows(c_me, e), cols], got.at[half_rows(c_me, e_me), cols],
                    s_sem, r_sem.at[q], e, t_me,
                )
            )

    def dispatch_far(q):
        dispatch(q, far, half_cols(q, z_odd), far_s, far_r)

    def dispatch_near(q):
        dispatch(q, near, pl.ds(*part_slice(q)), near_s, near_r)

    def landed(count, size, sem):
        here = got.at[pl.ds(0, count * half), pl.ds(0, size)]
        remote(here, here, sem, sem, e_me, partner).wait_recv()

    def forward(q, e, cols):
        here = got.at[half_rows(c_me, e), cols]
        start(remote(here, here, fwd_s, fwd_r.at[q], e_me, partner))

    def relay(q):
        cols = half_cols(q, z_odd)
        landed(len(far), part_slice(q)[1] // 2, far_r.at[q])
        for e in far:
            here = got.at[half_rows(c_me, e), cols]
            start(remote(here, here, rel_s, rel_r.at[q], e_me, z_pair * CORES + c_me))
            forward(q, e, cols)

    def forward_near(q):
        landed(len(near), part_slice(q)[1], near_r.at[q])
        for e in near:
            forward(q, e, pl.ds(*part_slice(q)))

    def forward_far(q):
        landed(len(far), part_slice(q)[1] // 2, rel_r.at[q])
        for e in far:
            forward(q, e, half_cols(q, 1 - z_odd))

    def forwarded(q):
        landed(ep - 1, part_slice(q)[1], fwd_r.at[q])

    dispatch_far(0)
    dispatch_far(1)
    for q in range(2, PARTS):
        pack_part(q)
        dispatch_far(q)
    loads[3].wait()
    loads[10].wait()
    norm_rows(xm, mix_gain, nm)
    loads[4].wait()
    loads[5].wait()
    rows = xm.shape[0]
    value_proj = jnp.dot(nm[...], vw[...], preferred_element_type=F32)
    inner_proj = jnp.dot(nm[...], iw[...], preferred_element_type=F32)
    gated[...] = (inner_proj * value_proj).astype(BF16)
    halo_copy = remote(
        gated.at[pl.ds(rows - 16, 16), :], halo, halo_s, halo_r,
        lax.rem(e_me + 1, ep), t_me,
    )
    halo_copy.start()
    dispatch_near(0)
    for q in range(1, PARTS):
        for c in expert_loads(q):
            c.start()
    loads[1].wait()
    loads[2].wait()
    lanes = (((1,), (1,)), ((), ()))
    row_scale = row_scales(xe)
    group_exp = jnp.exp(
        row_scale * lax.dot_general(ne[...], rg[...], lanes, preferred_element_type=F32)
    )
    expert_logit = row_scale * lax.dot_general(
        ne[...], rx[...], lanes, preferred_element_type=F32
    )
    groups, experts = group_exp.shape[1], expert_logit.shape[1]
    group = sum((picks[0] >= s * EPG).astype(jnp.int32) for s in range(1, groups))
    chosen_group = jnp.where(iota((count, groups), 1) == group, group_exp, 0.0)
    group_gate = jnp.sum(chosen_group, axis=1, keepdims=True) / jnp.sum(
        group_exp, axis=1, keepdims=True
    )
    expert_lane = iota((count, experts), 1)
    chosen = [
        jnp.exp(jnp.sum(jnp.where(expert_lane == p, expert_logit, 0.0), axis=1, keepdims=True))
        for p in picks
    ]
    scale = chosen[0] + chosen[1]
    w_lanes = [s * w_rows + (p - s * experts_here) for s, p in zip(shards, picks)]
    weights = sum(
        jnp.where(lane == at, group_gate * c / scale, 0.0) for at, c in zip(w_lanes, chosen)
    )
    scale_lanes = [s * w_rows + experts_here for s in shards]
    weights = weights + jnp.where(
        (lane == scale_lanes[0]) | (lane == scale_lanes[1]), row_scale, 0.0
    )

    def three_parts(value):
        parts = []
        for _ in range(3):
            parts.append(value.astype(BF16))
            value = value - parts[-1].astype(F32)
        return parts

    packed_w = sum(
        lax.dot_general(p, spread[...], (((0,), (0,)), ((), ())), preferred_element_type=F32)
        for p in three_parts(weights)
    )
    for e in range(ep):
        for c in range(CORES):
            wpack[e, :, c * half : (c + 1) * half] = packed_w[
                e * w_rows : (e + 1) * w_rows, c * span + e * half : c * span + (e + 1) * half
            ]
    wgot[e_me] = wpack[e_me]
    for c in range(CORES):
        got[half_rows(c, e_me), :] = pack[half_rows(c, e_me), :]

    for e in ep_peers:
        start(remote(wpack.at[e], wgot.at[e_me], w_s, w_r, e, t_me))
    for q in range(1, PARTS):
        dispatch_near(q)
    padded[8:, :] = gated[...].astype(F32)
    loads[6].wait()
    outer_proj = jnp.dot(nm[...], ow[...], preferred_element_type=F32)
    mix_share = rows // tp
    mix_rows = zs * mix_share
    everything = slice(None)
    pair_copy = remote(pair_out, pair_in, mp_s, mp_r, e_me, partner)

    def parity_rows(ref, c, step, cols):
        return jnp.concatenate(
            [
                ref[pl.ds(pl.multiple_of((z * CORES + c) * step, step), step), cols]
                for z in range(zs)
            ],
            axis=0,
        )

    def z_rows(z, step):
        return pl.ds(pl.multiple_of(z * step, step), step)

    def z_landed(blocks, ref, size, sem):
        here = ref.at[pl.ds(0, blocks), :, pl.ds(0, size)]
        remote(here, here, sem, sem, e_me, partner).wait_recv()

    def mixer_pair():
        halo_copy.wait()
        before = halo[...].astype(F32)[8:16, :]
        padded[0:8, :] = jnp.where(e_me > 0, before, jnp.zeros_like(before))
        loads[11].wait()
        n_taps = taps.shape[0]
        mixed = taps[0:1, :] * padded[pl.ds(9 - n_taps, rows), :]
        for j in range(1, n_taps):
            mixed = mixed + taps[j : j + 1, :] * padded[pl.ds(9 - n_taps + j, rows), :]
        conv[...] = (outer_proj * mixed).astype(BF16)

        loads[7].wait()

        ordered[0:mix_rows, :] = parity_rows(conv, c_no, mix_share, everything)
        ordered[mix_rows:, :] = parity_rows(conv, c_me, mix_share, everything)

        def mix_tile(cols):
            both = jnp.dot(ordered[...], mw[:, cols], preferred_element_type=F32)
            pair_out[:, cols] = both[0:mix_rows].astype(BF16)
            keep[:, cols] = both[mix_rows:]

        column_tiles(0, width // 2, 512, mix_tile)
        forward_near(0)
        forward_far(0)
        column_tiles(width // 2, width, 512, mix_tile)
        pair_copy.start()

    def mixer_sums():
        pair_copy.wait_recv()

        def sum_tile(cols):
            total = keep[:, cols] + pair_in[:, cols].astype(F32)
            keep[:, cols] = total
            pair_in[:, cols] = total.astype(BF16)

        column_tiles(0, width, 512, sum_tile)

        for z in z_peers:
            start(
                remote(
                    pair_in.at[z_rows(z, mix_share), :], zin.at[z_me], mz_s, mz_r,
                    e_me, z * CORES + c_me,
                )
            )

    def project(q):
        first, size = part_slice(q)
        cols = slice(first, first + size)

        for k in range(experts_here):
            if k == HOOK and q + 1 < PARTS:
                forward_near(q + 1)
                forward_far(q + 1)
            gate = jnp.dot(got[:, cols], gw[k, cols, :], preferred_element_type=F32)
            up = jnp.dot(got[:, cols], uw[k, cols, :], preferred_element_type=F32)
            if q:
                gate = gate + gate_acc[k]
                up = up + up_acc[k]
            if q < PARTS - 1:
                gate_acc[k] = gate
                up_acc[k] = up
                continue
            row = wrow[:, experts_here : experts_here + 1]
            gate = gate * row
            hid[:, k * hidden : (k + 1) * hidden] = (gate / (1.0 + jnp.exp(-gate)) * up * (row * wrow[:, k : k + 1])).astype(BF16)

    def arrived_weights():
        arrived = wgot.at[pl.ds(0, ep - 1)]
        remote(arrived, arrived, w_s, w_r, e_me, partner).wait_recv()
        across = jnp.concatenate(
            [wgot[e, :, c * half : (c + 1) * half] for c in range(CORES) for e in range(ep)], axis=1
        )
        square = (2 * span, 2 * span)
        same = jnp.where(iota(square, 0) == iota(square, 1), 1.0, 0.0).astype(BF16)
        wrow[...] = sum(
            lax.dot_general(same, p, lanes, preferred_element_type=F32)
            for p in three_parts(across)
        )

    for c in down_loads:
        c.start()
    for q in range(PARTS):
        relay(q)
    mixer_pair()
    for q in range(PARTS):
        if q == 0:
            arrived_weights()
        both_parts = gw.at[:, pl.ds(0, 2 * part_slice(q)[1]), :]
        pltpu.make_async_copy(both_parts, both_parts, expert_sem.at[q]).wait()
        forwarded(q)
        if q == 0:
            mixer_sums()
        project(q)
    pltpu.make_async_copy(dw, dw, down_sem).wait()

    chunk_unit = width // sum(CHUNKS)

    def chunk_cols(j):
        return slice(sum(CHUNKS[:j]) * chunk_unit, sum(CHUNKS[: j + 1]) * chunk_unit)

    def core_rows(c):
        return pl.ds(pl.multiple_of(c * span, span), span)

    y_copies = {}

    def stage_a(j):
        cols = chunk_cols(j)
        size = cols.stop - cols.start
        if j == 0:
            for c, dst in ((c_no, y_out), (c_me, y_keep)):
                part = jnp.dot(hid[core_rows(c), :], dw[:, cols], preferred_element_type=F32)
                dst[:, cols] = part.astype(dst.dtype)
                if dst is y_out:
                    y_copies[j] = remote(
                        y_out.at[:, cols], y_in.at[:, cols], yp_s, yp_r.at[j], e_me, partner
                    )
                    y_copies[j].start()
            return
        both_y[:, 0:size] = jnp.dot(hid[...], dw[:, cols], preferred_element_type=F32)
        y_out[:, cols] = both_y[core_rows(c_no), 0:size].astype(BF16)
        y_keep[:, cols] = both_y[core_rows(c_me), 0:size]
        y_copies[j] = remote(
            y_out.at[:, cols], y_in.at[:, cols], yp_s, yp_r.at[j], e_me, partner
        )
        y_copies[j].start()

    def e_rows(e):
        return pl.ds(pl.multiple_of(e * half, half), half)

    def stage_b(j):
        cols = chunk_cols(j)
        y_copies[j].wait_recv()
        y_in[:, cols] = (y_keep[:, cols] + y_in[:, cols].astype(F32)).astype(BF16)
        for e in far + near:
            start(
                remote(
                    y_in.at[e_rows(e), cols], e_in.at[e_rows(e_me), cols],
                    ye_s, ye_r.at[j], e, t_me,
                )
            )
        e_in[e_rows(e_me), cols] = y_in[e_rows(e_me), cols]

    def stage_c(j):
        cols = chunk_cols(j)
        size = cols.stop - cols.start
        here = e_in.at[pl.ds(0, (ep - 1) * half), pl.ds(0, size)]
        remote(here, here, ye_s, ye_r.at[j], e_me, partner).wait_recv()
        own = parity_rows(spread, c_me, share, core_rows(c_me))
        total = jnp.dot(own, e_in[:, cols], preferred_element_type=F32)
        s_out[:, cols] = total.astype(BF16)
        for z in z_peers:
            start(
                remote(
                    s_out.at[z_rows(z, share), cols], s_in.at[z_me, :, cols],
                    yz_s, yz_r.at[j], e_me, z * CORES + c_me,
                )
            )
        s_keep[:, cols] = total

    def stage_d(j):
        cols = chunk_cols(j)
        z_landed(zs - 1, s_in, cols.stop - cols.start, yz_r.at[j])
        total = s_keep[z_rows(z_me, share), cols]
        for z in z_peers:
            total = total + s_in[z, :, cols].astype(F32)
        expert_out[:, cols] = total.astype(BF16)

    def mixer_final():
        z_landed(zs - 1, zin, width, mz_r)
        total = keep[z_rows(z_me, mix_share), :]
        for z in z_peers:
            total = total + zin[z].astype(F32)
        mixer_out[...] = total.astype(BF16)

    lag_b, lag_c = LAGS
    chunks = len(CHUNKS)
    stages = [(stage_a, 0), (stage_b, lag_b), (stage_c, lag_c), (stage_d, lag_c + chunks)]
    for step in range(2 * chunks + lag_c):
        for stage, lag in stages:
            if 0 <= step - lag < chunks:
                stage(step - lag)
        if step == chunks + lag_c - 1:
            mixer_final()

    everything_sent = [
        (pack.at[pl.ds(0, len(near) * half), :], near_s),
        (pack.at[pl.ds(0, len(far) * half), pl.ds(0, width // 2)], far_s),
        (pack.at[pl.ds(0, len(far) * half), pl.ds(0, width // 2)], rel_s),
        (pack.at[pl.ds(0, (ep - 1) * half), :], fwd_s),
        (wpack.at[pl.ds(0, ep - 1)], w_s),
        (pair_out, mp_s),
        (zin.at[pl.ds(0, zs - 1)], mz_s),
        (y_out, yp_s),
        (y_in.at[pl.ds(0, (ep - 1) * half), :], ye_s),
        (s_in.at[pl.ds(0, zs - 1)], yz_s),
    ]
    for ref, sem in everything_sent:
        remote(ref, ref, sem, sem, e_me, partner).wait_send()


def store(a, b, a_out, b_out, sem):
    copies = [pltpu.make_async_copy(s, d, sem.at[i]) for i, (s, d) in enumerate(((a, a_out), (b, b_out)))]
    for c in copies:
        c.start()
    for c in copies:
        c.wait()


def local(ep, tp, *args):
    (mix_tokens, mix_gain, value_w, inner_w, outer_w, taps, mix_w, moe_tokens, moe_gain,
     router_group, router_expert, routes, gate_w, up_w, down_w) = args
    rows, width = mix_tokens.shape
    count = moe_tokens.shape[0]
    channels, hidden = value_w.shape[1], gate_w.shape[2]
    experts_here = gate_w.shape[0]
    zs = tp // CORES
    side = max(s for s in range(1, ep + 1) if ep % s == 0 and s * s <= ep)
    share, mix_share = count // tp, rows // tp
    topk = routes.shape[1]
    slots = experts_here * CAP
    if experts_here % EPG == 0:
        slots = slots // topk
    slots = min(slots, share)
    half = zs * slots
    span = ep * half
    w_rows, w_cols = -(-(experts_here + 1) // 8) * 8, -(-CORES * half // 128) * 128
    chunks = len(CHUNKS)
    chunk = width // sum(CHUNKS) * max(CHUNKS)
    any_ref = pl.BlockSpec(memory_space=pl.ANY)
    vmem = pl.BlockSpec(memory_space=pltpu.VMEM)
    V, D = pltpu.VMEM, lambda *s: pltpu.SemaphoreType.DMA(s)
    one = pltpu.SemaphoreType.DMA
    scratch = [
        V((1, width), F32), V(taps.shape, F32), V((1, width), F32), V(routes.T.shape, jnp.int32),
        V((rows, width), BF16), V((count, width), BF16),
        V(router_group.T.shape, BF16), V(router_expert.T.shape, BF16),
        V(value_w.shape, BF16), V(inner_w.shape, BF16), V(outer_w.shape, BF16),
        V(mix_w.shape, BF16),
        V(gate_w.shape, BF16), V(up_w.shape, BF16), V((experts_here * hidden, width), BF16),
        V((rows, width), BF16), V((count, width), BF16), V((count, 2 * span), BF16), V((2 * span, count), BF16),
        V((2 * span, width), BF16), V((2 * span, width), BF16),
        V((ep, w_rows, w_cols), F32), V((ep, w_rows, w_cols), F32), V((2 * span, w_rows), F32),
        V((rows, channels), BF16), V((16, channels), BF16), V((rows + 8, channels), F32),
        V((rows, channels), BF16), V((rows, channels), BF16),
        V((zs * mix_share, width), BF16), V((zs * mix_share, width), BF16),
        V((zs * mix_share, width), F32),
        V((zs, mix_share, width), BF16),
        V((experts_here, 2 * span, hidden), F32), V((experts_here, 2 * span, hidden), F32),
        V((2 * span, experts_here * hidden), BF16), V((2 * span, chunk), F32),
        V((span, width), BF16), V((span, width), BF16), V((span, width), F32),
        V((span, width), BF16),
        V((zs * share, width), F32), V((zs * share, width), BF16), V((zs, share, width), BF16),
        D(12), D(PARTS), one,
        one, D(PARTS), one, D(PARTS), one, D(PARTS), one, one, one, D(PARTS), one, one,
        one, one, one, one, one, D(chunks), one, D(chunks), one, D(chunks),
    ]
    out = [
        pltpu.VMEM((mix_share, width), BF16),
        pltpu.VMEM((share, width), BF16),
    ]
    in_specs = [any_ref] * len(args)
    results = pl.pallas_call(
        functools.partial(kernel, (ep, side, tp, zs, half, experts_here, w_rows)),
        out_shape=out,
        in_specs=in_specs,
        out_specs=[vmem, vmem],
        scratch_shapes=scratch,
        compiler_params=pltpu.CompilerParams(
            collective_id=0, has_side_effects=True, vmem_limit_bytes=65 * 1024 * 1000
        ),
        name="mixer_and_experts",
    )(
        mix_tokens, mix_gain.reshape(1, width), value_w, inner_w, outer_w, taps, mix_w,
        moe_tokens, moe_gain.reshape(1, width), router_group.T, router_expert.T, routes.T,
        gate_w, up_w, down_w,
    )
    return pl.pallas_call(
        store,
        out_shape=[jax.ShapeDtypeStruct(o.shape, BF16) for o in out],
        in_specs=[vmem, vmem],
        out_specs=[any_ref, any_ref],
        scratch_shapes=[D(2)],
        name="store",
    )(*[pltpu.with_memory_space_constraint(r, pltpu.VMEM) for r in results])


def solution(mesh):
    return jax.shard_map(
        lambda *args: tuple(local(mesh.shape["ep"], mesh.shape["tp"], *args)),
        mesh=mesh,
        in_specs=(
            P("ep", None), P(), P(None, "tp"), P(None, "tp"), P(None, "tp"), P(None, "tp"),
            P("tp", None), P("ep", None), P(), P(), P(), P("ep", None),
            P("ep", None, "tp"), P("ep", None, "tp"), P("ep", "tp", None),
        ),
        out_specs=(P(("ep", "tp"), None), P(("ep", "tp"), None)),
        check_vma=False,
    )
```

```python
import functools

import jax
import jax.numpy as jnp
from jax import lax
from jax.experimental import pallas as pl
from jax.experimental.pallas import tpu as pltpu
from jax.sharding import PartitionSpec as P

EPG = 4
CAP = 4
CORES = 2
CHUNKS = (1, 3, 4, 4, 4, 4, 4, 4, 2, 2)
LAGS = (1, 6)
SPLIT = (2, 2, 2, 2)
PARTS = len(SPLIT)
HOOK = 1
MESH = pl.DeviceIdType.MESH
F32, BF16 = jnp.float32, jnp.bfloat16


def iota(shape, dim):
    return lax.broadcasted_iota(jnp.int32, shape, dim)


def norm_rows(src, gain, dst):
    width = src.shape[1]

    def body(i, carry):
        rows = pl.ds(pl.multiple_of(i * 16, 16), 16)
        x = src[rows, :].astype(F32)
        inv = lax.rsqrt(jnp.sum(x * x, axis=1, keepdims=True) * (1.0 / width) + 1e-06)
        dst[rows, :] = (x * inv * gain[...]).astype(BF16)
        return carry

    lax.fori_loop(0, src.shape[0] // 16, body, 0, unroll=4)


def row_scales(src):
    width = src.shape[1]
    total = None
    for first in range(0, width, 512):
        x = src[:, first : first + 512].astype(F32)
        square = x * x
        total = square if total is None else total + square
    return lax.rsqrt(jnp.sum(total, axis=1, keepdims=True) * (1.0 / width) + 1e-06)


def column_tiles(first, last, tile, body):
    def step(i, carry):
        body(pl.ds(pl.multiple_of(i * tile, tile), tile))
        return carry

    lax.fori_loop(first // tile, last // tile, step, 0, unroll=4)


def kernel(
    cfg,
    mix_tokens, mix_gain_in, value_w, inner_w, outer_w, taps_in, mix_w, moe_tokens, moe_gain_in,
    router_group, router_expert, routes_in, gate_w, up_w, down_w,
    mixer_out, expert_out,
    mix_gain, taps, moe_gain, routes, xm, xe, rg, rx, vw, iw, ow, mw, gw, uw, dw,
    nm, ne, spread, gather, pack, got, wpack, wgot, wrow,
    gated, halo, padded, conv, ordered, pair_out, pair_in, keep, zin,
    gate_acc, up_acc, hid, both_y, y_out, y_in, y_keep, e_in, s_keep, s_out, s_in,
    load_sem, expert_sem, down_sem,
    near_s, near_r, far_s, far_r, rel_s, rel_r, w_s, w_r, fwd_s, fwd_r, halo_s, halo_r,
    mp_s, mp_r, mz_s, mz_r, yp_s, yp_r, ye_s, ye_r, yz_s, yz_r,
):
    ep, side, tp, zs, half, experts_here, w_rows = cfg
    e_me, t_me = lax.axis_index("ep"), lax.axis_index("tp")
    z_me, c_me = t_me // CORES, lax.rem(t_me, CORES)
    c_no = 1 - c_me
    partner = z_me * CORES + c_no
    width = xm.shape[1]
    tall = ep // side
    e_row, e_col = e_me // side, lax.rem(e_me, side)

    def placed(down, across):
        return lax.rem(e_row + down, tall) * side + lax.rem(e_col + across, side)

    near = [placed(d, 0) for d in range(1, tall)] + [placed(0, a) for a in range(1, side)]
    far = [placed(d, a) for d in range(1, tall) for a in range(1, side)]
    ep_peers = near + far
    z_odd = lax.rem(z_me, 2)
    z_pair = z_me + 1 - 2 * z_odd

    def z_flipped(bits):
        z = z_me
        for b in range(zs.bit_length() - 1):
            if bits >> b & 1:
                z = z + (1 - 2 * lax.rem(z_me // 2**b, 2)) * 2**b
        return z

    z_peers = [z_flipped(bits) for bits in range(zs - 1, 0, -1)]

    def start(copy):
        copy.start()

    barrier = pltpu.get_barrier_semaphore()
    for e in ep_peers:
        pl.semaphore_signal(barrier, inc=1, device_id={"ep": e, "tp": t_me}, device_id_type=MESH)
    for z in z_peers:
        pl.semaphore_signal(
            barrier, inc=1, device_id={"ep": e_me, "tp": z * CORES + c_me}, device_id_type=MESH
        )
    pl.semaphore_signal(barrier, inc=1, device_id={"ep": e_me, "tp": partner}, device_id_type=MESH)

    def load(k, src, dst):
        return pltpu.make_async_copy(src, dst, load_sem.at[k])

    loads = [
        load(k, s, d)
        for k, (s, d) in enumerate(
            [
                (moe_tokens, xe), (router_group, rg), (router_expert, rx), (mix_tokens, xm),
                (value_w, vw), (inner_w, iw), (outer_w, ow), (mix_w, mw),
                (routes_in, routes), (moe_gain_in, moe_gain), (mix_gain_in, mix_gain), (taps_in, taps),
            ]
        )
    ]
    unit = width // sum(SPLIT)

    def part_slice(q):
        return sum(SPLIT[:q]) * unit, SPLIT[q] * unit

    def expert_loads(q):
        rows = pl.ds(*part_slice(q))
        return [
            pltpu.make_async_copy(gate_w.at[:, rows, :], gw.at[:, rows, :], expert_sem.at[q]),
            pltpu.make_async_copy(up_w.at[:, rows, :], uw.at[:, rows, :], expert_sem.at[q]),
        ]

    hidden = down_w.shape[1]
    down_loads = [
        pltpu.make_async_copy(
            down_w.at[k], dw.at[k * hidden : (k + 1) * hidden, :], down_sem
        )
        for k in range(experts_here)
    ]
    for k in (8, 0, 9, 3, 10, 4, 5):
        loads[k].start()

    def remote(src, dst, s_sem, r_sem, e, t):
        return pltpu.make_async_remote_copy(
            src_ref=src, dst_ref=dst, send_sem=s_sem, recv_sem=r_sem,
            device_id={"ep": e, "tp": t}, device_id_type=MESH,
        )

    count = xe.shape[0]
    share = count // tp
    slots = half // zs
    span = ep * half
    loads[8].wait()
    diagonal = jnp.where(iota((count, count), 0) == iota((count, count), 1), 1.0, 0.0)
    r = lax.dot_general(
        diagonal.astype(BF16), routes[...].astype(F32).astype(BF16), (((1,), (1,)), ((), ())),
        preferred_element_type=F32,
    ).astype(jnp.int32)
    picks = [r[:, 0:1], r[:, 1:2]]
    lane = iota((count, -(-ep * w_rows // 128) * 128), 1)
    shards = [
        sum((p >= s * experts_here).astype(jnp.int32) for s in range(1, ep)) for p in picks
    ]
    member = jnp.where((lane == shards[0]) | (lane == shards[1]), 1.0, 0.0).astype(BF16)
    ti, tj = iota((count, count), 0), iota((count, count), 1)
    earlier = jnp.where(((ti ^ tj) < share) & (tj < ti), 1.0, 0.0).astype(BF16)
    rank = jnp.dot(earlier, member, preferred_element_type=F32)
    block = lax.shift_right_logical(iota((count, 1), 0), share.bit_length() - 1)
    base = (block & 1) * span + lax.shift_right_logical(block, 1) * slots
    slot_lane = iota((count, 2 * span), 1)
    hits = []
    for s in shards:
        mine = jnp.sum(jnp.where(lane == s, rank, 0.0), axis=1, keepdims=True).astype(jnp.int32)
        hits.append(slot_lane == base + s * half + mine)
    one_hot = jnp.where(hits[0] | hits[1], 1.0, 0.0).astype(BF16)
    spread[...] = one_hot
    gather[...] = lax.dot_general(
        one_hot, diagonal.astype(BF16), (((0,), (0,)), ((), ())), preferred_element_type=F32
    ).astype(BF16)
    loads[0].wait()
    loads[9].wait()

    def pack_part(q):
        first, size = part_slice(q)
        cols = slice(first, first + size)
        ne[:, cols] = (xe[:, cols].astype(F32) * moe_gain[:, cols]).astype(BF16)
        pack[:, cols] = jnp.dot(
            gather[...], ne[:, cols], preferred_element_type=F32
        ).astype(BF16)

    pack_part(0)
    pack_part(1)
    for k in (1, 2, 6, 11, 7):
        loads[k].start()
    for c in expert_loads(0):
        c.start()
    pl.semaphore_wait(barrier, (ep - 1) + (zs - 1) + 1)
    def half_rows(c, e):
        return pl.ds(pl.multiple_of(c * span + e * half, half), half)

    def half_cols(q, odd):
        first, size = part_slice(q)
        return pl.ds(pl.multiple_of(first + odd * (size // 2), 128), size // 2)

    def dispatch(q, peers, cols, s_sem, r_sem):
        for e in peers:
            start(
                remote(
                    pack.at[half_rows(c_me, e), cols], got.at[half_rows(c_me, e_me), cols],
                    s_sem, r_sem.at[q], e, t_me,
                )
            )

    def dispatch_far(q):
        dispatch(q, far, half_cols(q, z_odd), far_s, far_r)

    def dispatch_near(q):
        dispatch(q, near, pl.ds(*part_slice(q)), near_s, near_r)

    def landed(count, size, sem):
        here = got.at[pl.ds(0, count * half), pl.ds(0, size)]
        remote(here, here, sem, sem, e_me, partner).wait_recv()

    def forward(q, e, cols):
        here = got.at[half_rows(c_me, e), cols]
        start(remote(here, here, fwd_s, fwd_r.at[q], e_me, partner))

    def relay(q):
        cols = half_cols(q, z_odd)
        landed(len(far), part_slice(q)[1] // 2, far_r.at[q])
        for e in far:
            here = got.at[half_rows(c_me, e), cols]
            start(remote(here, here, rel_s, rel_r.at[q], e_me, z_pair * CORES + c_me))
            forward(q, e, cols)

    def forward_near(q):
        landed(len(near), part_slice(q)[1], near_r.at[q])
        for e in near:
            forward(q, e, pl.ds(*part_slice(q)))

    def forward_far(q):
        landed(len(far), part_slice(q)[1] // 2, rel_r.at[q])
        for e in far:
            forward(q, e, half_cols(q, 1 - z_odd))

    def forwarded(q):
        landed(ep - 1, part_slice(q)[1], fwd_r.at[q])

    dispatch_far(0)
    dispatch_far(1)
    for q in range(2, PARTS):
        pack_part(q)
        dispatch_far(q)
    loads[3].wait()
    loads[10].wait()
    norm_rows(xm, mix_gain, nm)
    loads[4].wait()
    loads[5].wait()
    rows = xm.shape[0]
    value_proj = jnp.dot(nm[...], vw[...], preferred_element_type=F32)
    inner_proj = jnp.dot(nm[...], iw[...], preferred_element_type=F32)
    gated[...] = (inner_proj * value_proj).astype(BF16)
    halo_copy = remote(
        gated.at[pl.ds(rows - 16, 16), :], halo, halo_s, halo_r,
        lax.rem(e_me + 1, ep), t_me,
    )
    halo_copy.start()
    dispatch_near(0)
    for q in range(1, PARTS):
        for c in expert_loads(q):
            c.start()
    loads[1].wait()
    loads[2].wait()
    lanes = (((1,), (1,)), ((), ()))
    row_scale = row_scales(xe)
    group_exp = jnp.exp(
        row_scale * lax.dot_general(ne[...], rg[...], lanes, preferred_element_type=F32)
    )
    expert_logit = row_scale * lax.dot_general(
        ne[...], rx[...], lanes, preferred_element_type=F32
    )
    groups, experts = group_exp.shape[1], expert_logit.shape[1]
    group = sum((picks[0] >= s * EPG).astype(jnp.int32) for s in range(1, groups))
    chosen_group = jnp.where(iota((count, groups), 1) == group, group_exp, 0.0)
    group_gate = jnp.sum(chosen_group, axis=1, keepdims=True) / jnp.sum(
        group_exp, axis=1, keepdims=True
    )
    expert_lane = iota((count, experts), 1)
    chosen = [
        jnp.exp(jnp.sum(jnp.where(expert_lane == p, expert_logit, 0.0), axis=1, keepdims=True))
        for p in picks
    ]
    scale = chosen[0] + chosen[1]
    w_lanes = [s * w_rows + (p - s * experts_here) for s, p in zip(shards, picks)]
    weights = sum(
        jnp.where(lane == at, group_gate * c / scale, 0.0) for at, c in zip(w_lanes, chosen)
    )
    scale_lanes = [s * w_rows + experts_here for s in shards]
    weights = weights + jnp.where(
        (lane == scale_lanes[0]) | (lane == scale_lanes[1]), row_scale, 0.0
    )

    def three_parts(value):
        parts = []
        for _ in range(3):
            parts.append(value.astype(BF16))
            value = value - parts[-1].astype(F32)
        return parts

    packed_w = sum(
        lax.dot_general(p, spread[...], (((0,), (0,)), ((), ())), preferred_element_type=F32)
        for p in three_parts(weights)
    )
    for e in range(ep):
        for c in range(CORES):
            wpack[e, :, c * half : (c + 1) * half] = packed_w[
                e * w_rows : (e + 1) * w_rows, c * span + e * half : c * span + (e + 1) * half
            ]
    wgot[e_me] = wpack[e_me]
    for c in range(CORES):
        got[half_rows(c, e_me), :] = pack[half_rows(c, e_me), :]

    for e in ep_peers:
        start(remote(wpack.at[e], wgot.at[e_me], w_s, w_r, e, t_me))
    for q in range(1, PARTS):
        dispatch_near(q)
    padded[8:, :] = gated[...].astype(F32)
    loads[6].wait()
    outer_proj = jnp.dot(nm[...], ow[...], preferred_element_type=F32)
    mix_share = rows // tp
    mix_rows = zs * mix_share
    everything = slice(None)
    pair_copy = remote(pair_out, pair_in, mp_s, mp_r, e_me, partner)

    def parity_rows(ref, c, step, cols):
        return jnp.concatenate(
            [
                ref[pl.ds(pl.multiple_of((z * CORES + c) * step, step), step), cols]
                for z in range(zs)
            ],
            axis=0,
        )

    def z_rows(z, step):
        return pl.ds(pl.multiple_of(z * step, step), step)

    def z_landed(blocks, ref, size, sem):
        here = ref.at[pl.ds(0, blocks), :, pl.ds(0, size)]
        remote(here, here, sem, sem, e_me, partner).wait_recv()

    def mixer_pair():
        halo_copy.wait()
        before = halo[...].astype(F32)[8:16, :]
        padded[0:8, :] = jnp.where(e_me > 0, before, jnp.zeros_like(before))
        loads[11].wait()
        n_taps = taps.shape[0]
        mixed = taps[0:1, :] * padded[pl.ds(9 - n_taps, rows), :]
        for j in range(1, n_taps):
            mixed = mixed + taps[j : j + 1, :] * padded[pl.ds(9 - n_taps + j, rows), :]
        conv[...] = (outer_proj * mixed).astype(BF16)

        loads[7].wait()

        ordered[0:mix_rows, :] = parity_rows(conv, c_no, mix_share, everything)
        ordered[mix_rows:, :] = parity_rows(conv, c_me, mix_share, everything)

        def mix_tile(cols):
            both = jnp.dot(ordered[...], mw[:, cols], preferred_element_type=F32)
            pair_out[:, cols] = both[0:mix_rows].astype(BF16)
            keep[:, cols] = both[mix_rows:]

        column_tiles(0, width // 2, 512, mix_tile)
        forward_near(0)
        forward_far(0)
        column_tiles(width // 2, width, 512, mix_tile)
        pair_copy.start()

    def mixer_sums():
        pair_copy.wait_recv()

        def sum_tile(cols):
            total = keep[:, cols] + pair_in[:, cols].astype(F32)
            keep[:, cols] = total
            pair_in[:, cols] = total.astype(BF16)

        column_tiles(0, width, 512, sum_tile)

        for z in z_peers:
            start(
                remote(
                    pair_in.at[z_rows(z, mix_share), :], zin.at[z_me], mz_s, mz_r,
                    e_me, z * CORES + c_me,
                )
            )

    def project(q):
        first, size = part_slice(q)
        cols = slice(first, first + size)

        for k in range(experts_here):
            if k == HOOK and q + 1 < PARTS:
                forward_near(q + 1)
                forward_far(q + 1)
            gate = jnp.dot(got[:, cols], gw[k, cols, :], preferred_element_type=F32)
            up = jnp.dot(got[:, cols], uw[k, cols, :], preferred_element_type=F32)
            if q:
                gate = gate + gate_acc[k]
                up = up + up_acc[k]
            if q < PARTS - 1:
                gate_acc[k] = gate
                up_acc[k] = up
                continue
            row = wrow[:, experts_here : experts_here + 1]
            gate = gate * row
            hid[:, k * hidden : (k + 1) * hidden] = (gate / (1.0 + jnp.exp(-gate)) * up * (row * wrow[:, k : k + 1])).astype(BF16)

    def arrived_weights():
        arrived = wgot.at[pl.ds(0, ep - 1)]
        remote(arrived, arrived, w_s, w_r, e_me, partner).wait_recv()
        across = jnp.concatenate(
            [wgot[e, :, c * half : (c + 1) * half] for c in range(CORES) for e in range(ep)], axis=1
        )
        square = (2 * span, 2 * span)
        same = jnp.where(iota(square, 0) == iota(square, 1), 1.0, 0.0).astype(BF16)
        wrow[...] = sum(
            lax.dot_general(same, p, lanes, preferred_element_type=F32)
            for p in three_parts(across)
        )

    for c in down_loads:
        c.start()
    for q in range(PARTS):
        relay(q)
    mixer_pair()
    for q in range(PARTS):
        if q == 0:
            arrived_weights()
        both_parts = gw.at[:, pl.ds(0, 2 * part_slice(q)[1]), :]
        pltpu.make_async_copy(both_parts, both_parts, expert_sem.at[q]).wait()
        forwarded(q)
        if q == 0:
            mixer_sums()
        project(q)
    pltpu.make_async_copy(dw, dw, down_sem).wait()

    chunk_unit = width // sum(CHUNKS)

    def chunk_cols(j):
        return slice(sum(CHUNKS[:j]) * chunk_unit, sum(CHUNKS[: j + 1]) * chunk_unit)

    def core_rows(c):
        return pl.ds(pl.multiple_of(c * span, span), span)

    y_copies = {}

    def stage_a(j):
        cols = chunk_cols(j)
        size = cols.stop - cols.start
        if j == 0:
            for c, dst in ((c_no, y_out), (c_me, y_keep)):
                part = jnp.dot(hid[core_rows(c), :], dw[:, cols], preferred_element_type=F32)
                dst[:, cols] = part.astype(dst.dtype)
                if dst is y_out:
                    y_copies[j] = remote(
                        y_out.at[:, cols], y_in.at[:, cols], yp_s, yp_r.at[j], e_me, partner
                    )
                    y_copies[j].start()
            return
        both_y[:, 0:size] = jnp.dot(hid[...], dw[:, cols], preferred_element_type=F32)
        y_out[:, cols] = both_y[core_rows(c_no), 0:size].astype(BF16)
        y_keep[:, cols] = both_y[core_rows(c_me), 0:size]
        y_copies[j] = remote(
            y_out.at[:, cols], y_in.at[:, cols], yp_s, yp_r.at[j], e_me, partner
        )
        y_copies[j].start()

    def e_rows(e):
        return pl.ds(pl.multiple_of(e * half, half), half)

    def stage_b(j):
        cols = chunk_cols(j)
        y_copies[j].wait_recv()
        y_in[:, cols] = (y_keep[:, cols] + y_in[:, cols].astype(F32)).astype(BF16)
        for e in far + near:
            start(
                remote(
                    y_in.at[e_rows(e), cols], e_in.at[e_rows(e_me), cols],
                    ye_s, ye_r.at[j], e, t_me,
                )
            )
        e_in[e_rows(e_me), cols] = y_in[e_rows(e_me), cols]

    def stage_c(j):
        cols = chunk_cols(j)
        size = cols.stop - cols.start
        here = e_in.at[pl.ds(0, (ep - 1) * half), pl.ds(0, size)]
        remote(here, here, ye_s, ye_r.at[j], e_me, partner).wait_recv()
        own = parity_rows(spread, c_me, share, core_rows(c_me))
        total = jnp.dot(own, e_in[:, cols], preferred_element_type=F32)
        s_out[:, cols] = total.astype(BF16)
        for z in z_peers:
            start(
                remote(
                    s_out.at[z_rows(z, share), cols], s_in.at[z_me, :, cols],
                    yz_s, yz_r.at[j], e_me, z * CORES + c_me,
                )
            )
        s_keep[:, cols] = total

    def stage_d(j):
        cols = chunk_cols(j)
        z_landed(zs - 1, s_in, cols.stop - cols.start, yz_r.at[j])
        total = s_keep[z_rows(z_me, share), cols]
        for z in z_peers:
            total = total + s_in[z, :, cols].astype(F32)
        expert_out[:, cols] = total.astype(BF16)

    def mixer_final():
        z_landed(zs - 1, zin, width, mz_r)
        total = keep[z_rows(z_me, mix_share), :]
        for z in z_peers:
            total = total + zin[z].astype(F32)
        mixer_out[...] = total.astype(BF16)

    lag_b, lag_c = LAGS
    chunks = len(CHUNKS)
    stages = [(stage_a, 0), (stage_b, lag_b), (stage_c, lag_c), (stage_d, lag_c + chunks)]
    for step in range(2 * chunks + lag_c):
        for stage, lag in stages:
            if 0 <= step - lag < chunks:
                stage(step - lag)
        if step == chunks + lag_c - 1:
            mixer_final()

    everything_sent = [
        (pack.at[pl.ds(0, len(near) * half), :], near_s),
        (pack.at[pl.ds(0, len(far) * half), pl.ds(0, width // 2)], far_s),
        (pack.at[pl.ds(0, len(far) * half), pl.ds(0, width // 2)], rel_s),
        (pack.at[pl.ds(0, (ep - 1) * half), :], fwd_s),
        (wpack.at[pl.ds(0, ep - 1)], w_s),
        (pair_out, mp_s),
        (zin.at[pl.ds(0, zs - 1)], mz_s),
        (y_out, yp_s),
        (y_in.at[pl.ds(0, (ep - 1) * half), :], ye_s),
        (s_in.at[pl.ds(0, zs - 1)], yz_s),
    ]
    for ref, sem in everything_sent:
        remote(ref, ref, sem, sem, e_me, partner).wait_send()


def store(a, b, a_out, b_out, sem):
    copies = [pltpu.make_async_copy(s, d, sem.at[i]) for i, (s, d) in enumerate(((a, a_out), (b, b_out)))]
    for c in copies:
        c.start()
    for c in copies:
        c.wait()


def local(ep, tp, *args):
    (mix_tokens, mix_gain, value_w, inner_w, outer_w, taps, mix_w, moe_tokens, moe_gain,
     router_group, router_expert, routes, gate_w, up_w, down_w) = args
    rows, width = mix_tokens.shape
    count = moe_tokens.shape[0]
    channels, hidden = value_w.shape[1], gate_w.shape[2]
    experts_here = gate_w.shape[0]
    zs = tp // CORES
    side = max(s for s in range(1, ep + 1) if ep % s == 0 and s * s <= ep)
    share, mix_share = count // tp, rows // tp
    topk = routes.shape[1]
    slots = experts_here * CAP
    if experts_here % EPG == 0:
        slots = slots // topk
    slots = min(slots, share)
    half = zs * slots
    span = ep * half
    w_rows, w_cols = -(-(experts_here + 1) // 8) * 8, -(-CORES * half // 128) * 128
    chunks = len(CHUNKS)
    chunk = width // sum(CHUNKS) * max(CHUNKS)
    any_ref = pl.BlockSpec(memory_space=pl.ANY)
    vmem = pl.BlockSpec(memory_space=pltpu.VMEM)
    V, D = pltpu.VMEM, lambda *s: pltpu.SemaphoreType.DMA(s)
    one = pltpu.SemaphoreType.DMA
    scratch = [
        V((1, width), F32), V(taps.shape, F32), V((1, width), F32), V(routes.T.shape, jnp.int32),
        V((rows, width), BF16), V((count, width), BF16),
        V(router_group.T.shape, BF16), V(router_expert.T.shape, BF16),
        V(value_w.shape, BF16), V(inner_w.shape, BF16), V(outer_w.shape, BF16),
        V(mix_w.shape, BF16),
        V(gate_w.shape, BF16), V(up_w.shape, BF16), V((experts_here * hidden, width), BF16),
        V((rows, width), BF16), V((count, width), BF16), V((count, 2 * span), BF16), V((2 * span, count), BF16),
        V((2 * span, width), BF16), V((2 * span, width), BF16),
        V((ep, w_rows, w_cols), F32), V((ep, w_rows, w_cols), F32), V((2 * span, w_rows), F32),
        V((rows, channels), BF16), V((16, channels), BF16), V((rows + 8, channels), F32),
        V((rows, channels), BF16), V((rows, channels), BF16),
        V((zs * mix_share, width), BF16), V((zs * mix_share, width), BF16),
        V((zs * mix_share, width), F32),
        V((zs, mix_share, width), BF16),
        V((experts_here, 2 * span, hidden), F32), V((experts_here, 2 * span, hidden), F32),
        V((2 * span, experts_here * hidden), BF16), V((2 * span, chunk), F32),
        V((span, width), BF16), V((span, width), BF16), V((span, width), F32),
        V((span, width), BF16),
        V((zs * share, width), F32), V((zs * share, width), BF16), V((zs, share, width), BF16),
        D(12), D(PARTS), one,
        one, D(PARTS), one, D(PARTS), one, D(PARTS), one, one, one, D(PARTS), one, one,
        one, one, one, one, one, D(chunks), one, D(chunks), one, D(chunks),
    ]
    out = [
        pltpu.VMEM((mix_share, width), BF16),
        pltpu.VMEM((share, width), BF16),
    ]
    in_specs = [any_ref] * len(args)
    results = pl.pallas_call(
        functools.partial(kernel, (ep, side, tp, zs, half, experts_here, w_rows)),
        out_shape=out,
        in_specs=in_specs,
        out_specs=[vmem, vmem],
        scratch_shapes=scratch,
        compiler_params=pltpu.CompilerParams(
            collective_id=0, has_side_effects=True, vmem_limit_bytes=65 * 1024 * 1000
        ),
        name="mixer_and_experts",
    )(
        mix_tokens, mix_gain.reshape(1, width), value_w, inner_w, outer_w, taps, mix_w,
        moe_tokens, moe_gain.reshape(1, width), router_group.T, router_expert.T, routes.T,
        gate_w, up_w, down_w,
    )
    return pl.pallas_call(
        store,
        out_shape=[jax.ShapeDtypeStruct(o.shape, BF16) for o in out],
        in_specs=[vmem, vmem],
        out_specs=[any_ref, any_ref],
        scratch_shapes=[D(2)],
        name="store",
    )(*[pltpu.with_memory_space_constraint(r, pltpu.VMEM) for r in results])


def solution(mesh):
    return jax.shard_map(
        lambda *args: tuple(local(mesh.shape["ep"], mesh.shape["tp"], *args)),
        mesh=mesh,
        in_specs=(
            P("ep", None), P(), P(None, "tp"), P(None, "tp"), P(None, "tp"), P(None, "tp"),
            P("tp", None), P("ep", None), P(), P(), P(), P("ep", None),
            P("ep", None, "tp"), P("ep", None, "tp"), P("ep", "tp", None),
        ),
        out_specs=(P(("ep", "tp"), None), P(("ep", "tp"), None)),
        check_vma=False,
    )
```
